256 devices in a mesh: kv: 32 (over z, x), tp: 8 (over y, core).
Axes of the slice: x: 4, y: 4, z: 8, core: 2. Of those that a mesh axis runs over, the one named last changes fastest.
Arguments:
- tokens: bfloat16 [32768, 2048], P('kv'), may hold values from -72 to 72
- query_weight: bfloat16 [2048, 2048], P(None, 'tp'), may hold values from -0.125 to 0.125
- key_projection_matrix: bfloat16 [2048, 1024], P(None, 'tp'), may hold values from -0.125 to 0.125
- value_projection_matrix: bfloat16 [2048, 1024], P(None, 'tp'), may hold values from -0.125 to 0.125
- out_weight: bfloat16 [2048, 2048], P('tp'), may hold values from -1.5 to 1.5
- chosen: int32 [256, 12], P('kv'), may hold values from -1 to 1023, as said below
Outputs:
- layer_out: bfloat16 [32768, 2048], P(('kv', 'tp'))
The draws below stay inside these ranges and needn't reach their ends.
Inputs may be any that keep to these rules, and one draw needn't show every extreme that they name: `chosen`: positions are grouped in consecutive groups of 1024. The blocks named in one row lie in distinct groups, all earlier than the group of the row's query block; a query block in group g has exactly min(12, g) entries that are not -1, first in its row, and the rest are -1. So the query blocks of one group name at most 8 blocks of any one other group, and in every draw some group's query blocks all name blocks of one same earlier group.
All inputs are finite; a program needn't handle non-finite values.
Results may differ from the reference program's by a relative error of at most 0.014.
The reference program's roundings to bfloat16 on the way count: a program that leaves them out, or rounds other values in their place, can miss the bound.
Values may be sent and summed in bfloat16 or wider, within the bound.
A program may use at most 64 MiB of HBM per device.

```python
import jax
import jax.numpy as jnp
from jax import lax

MODEL_WIDTH = 2048
QUERY_HEADS = 16
KEY_VALUE_HEADS = 8
HEAD_SIZE = 128
TOK_DEV = 1024
QUERY_BLOCK_SPAN = 128
KEY_BLOCK_SPAN = 32
NFAR = 12
SEQUENCE_TOKENS = 32768
N_TP = 8


def draw_tokens(key, part):
    split_keys = jax.random.split(jax.random.fold_in(key, 11), 3)
    base_rows = jnp.clip(jax.random.normal(split_keys[0], (SEQUENCE_TOKENS, MODEL_WIDTH), jnp.float32), -6.0, 6.0)
    return base_rows.astype(jnp.bfloat16)


def draw_chosen(key, part):
    group_count = SEQUENCE_TOKENS // TOK_DEV
    per_group = TOK_DEV // QUERY_BLOCK_SPAN
    blocks_per_group = TOK_DEV // KEY_BLOCK_SPAN
    query_count = SEQUENCE_TOKENS // QUERY_BLOCK_SPAN
    split_keys = jax.random.split(jax.random.fold_in(key, 7), 4)
    owner_ids = jnp.arange(group_count, dtype=jnp.int32)
    home_group = jnp.arange(query_count, dtype=jnp.int32) // per_group
    first_local = jnp.arange(query_count, dtype=jnp.int32) % per_group == 0
    popular = jax.random.randint(split_keys[0], (group_count,), 0, 3) * (1 << 19)
    jitter = jax.random.randint(split_keys[1], (query_count, group_count), 0, 1 << 20)
    favoured = jax.random.randint(split_keys[2], (group_count,), 0, 1 << 20) % jnp.maximum(owner_ids, 1)
    source = home_group[:, None]
    target = owner_ids[None, :]
    forced = (target == favoured[home_group][:, None]) | first_local[:, None] & ((target == source - 1) | (target == source - group_count // 2))
    ranking = (jitter + popular[None, :]) * group_count + target
    ranking = jnp.where(forced, ranking + (1 << 29), ranking)
    ranking = jnp.where(target < source, ranking, -1)
    take_count = min(NFAR, group_count)
    best_scores, picked_owner = lax.top_k(ranking, take_count)
    inner_ids = jax.random.randint(split_keys[3], (query_count, take_count), 0, blocks_per_group)
    listed = jnp.where(best_scores >= 0, picked_owner.astype(jnp.int32) * blocks_per_group + inner_ids, -1)
    if take_count < NFAR:
        padding = jnp.full((query_count, NFAR - take_count), -1, jnp.int32)
        listed = jnp.concatenate([listed, padding], axis=1)
    return listed.astype(jnp.int32)


def steps_of(own_key, extent, cuts, smallest, high):
    def one(axis_at, shards_of):
        heights = jax.random.uniform(jax.random.fold_in(jax.random.fold_in(own_key, 6), axis_at), (shards_of,), jnp.float32, smallest / len(cuts), high / len(cuts))
        return jnp.repeat(jnp.exp(heights), extent[axis_at] // shards_of).reshape((-1,) + (1,) * (len(extent) - axis_at - 1))

    loudness = one(*cuts[0])
    for cut in cuts[1:]:
        loudness = loudness * one(*cut)
    return loudness


def bell_draw(rng, dims, scale, reach, pieces=(), kind=jnp.bfloat16):
    result = scale * jax.random.normal(rng, dims, jnp.float32)
    if pieces:
        result = result * steps_of(rng, dims, pieces, -0.22, 0.18)
    return jnp.clip(result, -reach, reach).astype(kind)


def setup_inputs(seed: int = 0) -> dict:
    arg_keys = jax.random.split(jax.random.key(seed), 7)
    return {
        "tokens": draw_tokens(jax.random.fold_in(arg_keys[6], 71), 0),
        "query_weight": bell_draw(arg_keys[1], (MODEL_WIDTH, QUERY_HEADS * HEAD_SIZE), MODEL_WIDTH ** -0.5, 0.125, ((1, 8),)),
        "key_projection_matrix": bell_draw(arg_keys[2], (MODEL_WIDTH, KEY_VALUE_HEADS * HEAD_SIZE), MODEL_WIDTH ** -0.5, 0.125, ((1, 8),)),
        "value_projection_matrix": bell_draw(arg_keys[3], (MODEL_WIDTH, KEY_VALUE_HEADS * HEAD_SIZE), MODEL_WIDTH ** -0.5, 0.125, ((1, 8),)),
        "out_weight": bell_draw(arg_keys[4], (QUERY_HEADS * HEAD_SIZE, MODEL_WIDTH), (HEAD_SIZE // 8) ** -0.5, 1.5, ((0, 8),)),
        "chosen": draw_chosen(jax.random.fold_in(arg_keys[6], 71), 0),
    }


def reference(tokens, query_weight, key_projection_matrix, value_projection_matrix, out_weight, chosen):
    queries = jnp.dot(tokens, query_weight, preferred_element_type=jnp.float32).astype(jnp.bfloat16)
    key_vectors = jnp.dot(tokens, key_projection_matrix, preferred_element_type=jnp.float32).astype(jnp.bfloat16)
    value_vectors = jnp.dot(tokens, value_projection_matrix, preferred_element_type=jnp.float32).astype(jnp.bfloat16)
    grouped_head_index = QUERY_HEADS // KEY_VALUE_HEADS
    diag_blocks = QUERY_BLOCK_SPAN // KEY_BLOCK_SPAN
    blocked_keys = key_vectors.reshape(SEQUENCE_TOKENS // KEY_BLOCK_SPAN, KEY_BLOCK_SPAN, KEY_VALUE_HEADS * HEAD_SIZE)
    blocked_values = value_vectors.reshape(SEQUENCE_TOKENS // KEY_BLOCK_SPAN, KEY_BLOCK_SPAN, KEY_VALUE_HEADS * HEAD_SIZE)
    offsets = jnp.arange(KEY_BLOCK_SPAN, dtype=jnp.int32)
    row_ids = jnp.arange(QUERY_BLOCK_SPAN, dtype=jnp.int32)

    def one_block(block_index):
        first_row = block_index * QUERY_BLOCK_SPAN
        queries_in_block = lax.dynamic_slice_in_dim(queries, first_row, QUERY_BLOCK_SPAN, 0)
        queries_in_block = queries_in_block.reshape(QUERY_BLOCK_SPAN, KEY_VALUE_HEADS, grouped_head_index, HEAD_SIZE).astype(jnp.float32)
        picked = lax.dynamic_slice_in_dim(chosen, block_index, 1, 0)[0]
        block_ids = jnp.concatenate([block_index * diag_blocks + jnp.arange(diag_blocks, dtype=jnp.int32), picked])
        is_valid = block_ids >= 0
        guarded_block_index = jnp.maximum(block_ids, 0)
        key_pos = (guarded_block_index[:, None] * KEY_BLOCK_SPAN + offsets[None, :]).reshape(-1)
        key_ok = jnp.broadcast_to(is_valid[:, None], (block_ids.shape[0], KEY_BLOCK_SPAN)).reshape(-1)
        query_pos = first_row + row_ids
        allowed = key_ok[None, :] & (key_pos[None, :] <= query_pos[:, None])
        nearby_keys = blocked_keys[guarded_block_index].reshape(-1, KEY_VALUE_HEADS, HEAD_SIZE).astype(jnp.float32)
        nearby_values = blocked_values[guarded_block_index].reshape(-1, KEY_VALUE_HEADS, HEAD_SIZE).astype(jnp.float32)
        scores = jnp.einsum("qgrd,kgd->grqk", queries_in_block, nearby_keys, precision=lax.Precision.HIGHEST) * (HEAD_SIZE ** -0.5)
        scores = jnp.where(allowed[None, None], scores, -jnp.inf)
        row_max = jnp.max(scores, axis=-1, keepdims=True)
        exp_scores = jnp.exp(scores - row_max)
        row_sum = jnp.sum(exp_scores, axis=-1, keepdims=True)
        weights = (exp_scores / row_sum).astype(jnp.bfloat16)
        mixed = jnp.einsum("grqk,kgd->qgrd", weights.astype(jnp.float32), nearby_values, precision=lax.Precision.HIGHEST)
        return mixed.astype(jnp.bfloat16).reshape(QUERY_BLOCK_SPAN, QUERY_HEADS * HEAD_SIZE)

    all_blocks = lax.map(one_block, jnp.arange(SEQUENCE_TOKENS // QUERY_BLOCK_SPAN, dtype=jnp.int32))
    attended = all_blocks.reshape(SEQUENCE_TOKENS, QUERY_HEADS * HEAD_SIZE)
    slice_width = QUERY_HEADS * HEAD_SIZE // N_TP
    summed = jnp.zeros((SEQUENCE_TOKENS, MODEL_WIDTH), jnp.float32)
    for part_index in range(N_TP):
        lower = part_index * slice_width
        partial_value = jnp.dot(attended[:, lower:lower + slice_width], out_weight[lower:lower + slice_width],
                          preferred_element_type=jnp.float32)
        rounded = lax.optimization_barrier(partial_value.astype(jnp.bfloat16))
        summed = summed + rounded.astype(jnp.float32)
    return summed.astype(jnp.bfloat16)
```

```python
import functools

import jax
import jax.numpy as jnp
from jax import lax
from jax.experimental import pallas as pl
from jax.experimental.pallas import tpu as pltpu
from jax.sharding import PartitionSpec as P

MESH = pl.DeviceIdType.MESH
NZ, NX, NY, NC = 8, 4, 4, 2
TP = NY * NC
HALF = NZ // 2
HEAD = 128
SPAN = 128
KSPAN = 32
NFAR = 12
TOK = 1024
NBLK = TOK // KSPAN
NQB = TOK // SPAN
WIDTH = 2048
QW = 256
GROUPS = NZ * NX
LISTED = SPAN + NFAR * KSPAN
CHUNK = 256
NCHUNK = TOK // CHUNK
SCALE = HEAD ** (-0.5)
K, V = 0, 1
UP = [(K, j) for j in range(1, HALF + 1)] + [(V, j) for j in range(1, HALF)]
DOWN = [(K, j) for j in range(1, HALF)] + [(V, j) for j in range(1, HALF + 1)]


def kernel(
    tok_h, wq_h, wk_h, wv_h, wo_h, chosen_v, chosen_s,
    out_ref,
    x_v, w_v, wfull, q_v, own_k, own_v, up_bufs, dn_bufs, uni_k, uni_v, stage,
    tab_v, tab_s, kb, vb, att, att_all, acc,
    tok_sem, w_sem, wo_sem, tab_send, tab_recv, tab_loc,
    up_send, up_recv, dn_send, dn_recv, x_send, x_recv,
    wy_send, wy_recv, wd_send, wd_recv, att_send, att_recv,
):
    kv = lax.axis_index("kv")
    tp = lax.axis_index("tp")
    z, x = kv // NX, kv % NX
    y, c = tp // NC, tp % NC

    def at_z(step):
        return {"kv": ((z + step + NZ) % NZ) * NX + x, "tp": tp}

    def at_x(step):
        return {"kv": z * NX + (x + step + NX) % NX, "tp": tp}

    def at_tp(index):
        return {"kv": kv, "tp": index}

    def tp_of(dy, dc):
        return ((y + dy + NY) % NY) * NC + (c + dc) % NC

    bar = pltpu.get_barrier_semaphore()
    for dev in [at_z(1), at_z(-1)] + [at_x(d) for d in range(1, NX)]:
        pl.semaphore_signal(bar, inc=1, device_id=dev, device_id_type=MESH)
    for d in range(1, TP):
        pl.semaphore_signal(bar, inc=1, device_id=at_tp((tp + d) % TP), device_id_type=MESH)

    def rows(i):
        return pl.ds(pl.multiple_of(i * CHUNK, CHUNK), CHUNK)

    def tok_copy(i):
        return pltpu.make_async_copy(tok_h.at[rows(i)], x_v.at[rows(i)], tok_sem.at[i])

    w_copies = [
        pltpu.make_async_copy(wk_h, w_v.at[:, 0:128], w_sem.at[0]),
        pltpu.make_async_copy(wv_h, w_v.at[:, 128:256], w_sem.at[1]),
        pltpu.make_async_copy(wq_h, w_v.at[:, 256:512], w_sem.at[2]),
    ]
    w_copies[0].start()
    w_copies[1].start()
    for i in range(NCHUNK):
        tok_copy(i).start()
    wo_copy = pltpu.make_async_copy(wo_h, wfull.at[tp], wo_sem.at[0])
    wo_copy.start()
    w_copies[2].start()

    lane = lax.broadcasted_iota(jnp.int32, (NQB, 128), 1)
    table = jnp.zeros((NQB, 128), jnp.int32)
    listed = chosen_v[...]
    for j in range(NFAR):
        col = jnp.broadcast_to(listed[:, j : j + 1], (NQB, 128))
        table = table + jnp.where((col >= 0) & ((col >> 5) == lane), col & (NBLK - 1), 0)
    tab_v[0] = table

    pl.semaphore_wait(bar, 2 + NX - 1 + TP - 1)

    def tab_copy(d):
        return pltpu.make_async_remote_copy(
            src_ref=tab_v.at[0], dst_ref=tab_v.at[d], send_sem=tab_send.at[d], recv_sem=tab_recv.at[d],
            device_id=at_x(d), device_id_type=MESH,
        )

    def tab_to_smem(d):
        return pltpu.make_async_copy(tab_v.at[d], tab_s.at[d], tab_loc.at[d])

    for d in range(1, NX):
        tab_copy(d).start()
    tab_to_smem(0).start()

    def wy(slot, sem, dy, lo, hi):
        ref = wfull.at[slot, lo:hi]
        return pltpu.make_async_remote_copy(
            src_ref=ref, dst_ref=ref, send_sem=wy_send.at[sem], recv_sem=wy_recv.at[sem],
            device_id=at_tp(tp_of(dy, 0)), device_id_type=MESH,
        )

    def wd(slot, sem, lo, hi):
        ref = wfull.at[slot, lo:hi]
        return pltpu.make_async_remote_copy(
            src_ref=ref, dst_ref=ref, send_sem=wd_send.at[sem], recv_sem=wd_recv.at[sem],
            device_id=at_tp(tp_of(0, 1)), device_id_type=MESH,
        )

    y_sends = [(tp, 0, 1, 0, QW), (tp, 1, -1, 0, QW), (tp_of(-1, 0), 2, 1, 0, QW // 2), (tp_of(1, 0), 3, -1, QW // 2, QW)]
    y_recvs = [
        (tp_of(-1, 0), 0, 1, 0, QW), (tp_of(1, 0), 1, -1, 0, QW),
        (tp_of(2, 0), 2, 1, 0, QW // 2), (tp_of(2, 0), 3, -1, QW // 2, QW),
    ]
    d_rows = [(0, QW), (0, QW), (0, QW), (0, QW // 2), (QW // 2, QW)]
    d_sends = [(s, i) + d_rows[i] for i, s in enumerate([tp, tp_of(-1, 0), tp_of(1, 0), tp_of(2, 0), tp_of(2, 0)])]
    d_recvs = [(s, i) + d_rows[i] for i, s in enumerate([tp_of(0, 1), tp_of(-1, 1), tp_of(1, 1), tp_of(2, 1), tp_of(2, 1)])]
    wo_copy.wait()
    wy(*y_sends[0]).start()
    wy(*y_sends[1]).start()
    wd(*d_sends[0]).start()

    w_copies[0].wait()
    w_copies[1].wait()

    def project_kv(i, carry):
        tok_copy(i).wait()
        pair = jnp.dot(x_v[rows(i)], w_v[:, 0:256], preferred_element_type=jnp.float32).astype(jnp.bfloat16)
        blocks = pl.ds(i * (CHUNK // KSPAN), CHUNK // KSPAN)
        own_k[blocks] = pair[:, :HEAD].reshape(CHUNK // KSPAN, KSPAN, HEAD)
        own_v[blocks] = pair[:, HEAD:].reshape(CHUNK // KSPAN, KSPAN, HEAD)
        return carry

    lax.fori_loop(0, NCHUNK, project_kv, 0)
    own = {K: own_k, V: own_v}
    up_ref = {(p, j): up_bufs[i] for i, (p, j) in enumerate(UP)}
    dn_ref = {(p, j): dn_bufs[i] for i, (p, j) in enumerate(DOWN)}
    uni = {K: uni_k, V: uni_v}

    def up_copy(p, j):
        src = own[p] if j == 1 else up_ref[p, j - 1]
        return pltpu.make_async_remote_copy(
            src_ref=src, dst_ref=up_ref[p, j], send_sem=up_send.at[p, j], recv_sem=up_recv.at[p, j],
            device_id=at_z(1), device_id_type=MESH,
        )

    def dn_copy(p, j):
        src = own[p] if j == 1 else dn_ref[p, j - 1]
        return pltpu.make_async_remote_copy(
            src_ref=src, dst_ref=dn_ref[p, j], send_sem=dn_send.at[p, j], recv_sem=dn_recv.at[p, j],
            device_id=at_z(-1), device_id_type=MESH,
        )

    def up_arrives(p, j, here):
        return (here - j >= 0) & (here <= NZ - 1)

    def dn_arrives(p, j, here):
        first = (here + j) % NZ
        return first <= (HALF - 2 if p == K else HALF - 1)

    def send_up(p, j):
        if (p, j) in up_ref:
            @pl.when(up_arrives(p, j, z + 1))
            def _():
                up_copy(p, j).start()

    def send_down(p, j):
        if (p, j) in dn_ref:
            @pl.when(dn_arrives(p, j, (z + NZ - 1) % NZ))
            def _():
                dn_copy(p, j).start()

    def stage_rows(a, p, d):
        return ((a * 2 + p) * (NX - 1) + d - 1) * NQB

    def x_copy(a, p, d, source, sender_x):
        group_rows = pl.ds((source * NX + sender_x) * NQB, NQB)
        return pltpu.make_async_remote_copy(
            src_ref=stage.at[pl.ds(stage_rows(a, p, d), NQB)],
            dst_ref=uni[p].at[group_rows],
            send_sem=x_send.at[a, p, d - 1], recv_sem=x_recv.at[a, p, d - 1],
            device_id=at_x(d), device_id_type=MESH,
        )

    def spread(a, p, buf, source, mine):
        group = source * NX + x

        def pick(b, carry):
            for d in range(1, NX):
                stage[stage_rows(a, p, d) + b] = buf[tab_s[NX - d, b, group]]
            if mine:
                uni[p][group * NQB + b] = buf[tab_s[0, b, group]]
            return carry

        lax.fori_loop(0, NQB, pick, 0)
        for d in range(1, NX):
            if mine:
                x_copy(a, p, d, source, x).start()
            else:
                @pl.when(x + d < NX)
                def _():
                    x_copy(a, p, d, source, x).start()

    for p in (K, V):
        send_up(p, 1)
        send_down(p, 1)

    for d in range(1, NX):
        tab_copy(d).wait_recv()
        tab_to_smem(d).start()
    for d in range(NX):
        tab_to_smem(d).wait()

    spread(0, K, own_k, z, False)
    spread(0, V, own_v, z, False)

    w_copies[2].wait()

    def project_q(i, carry):
        q_v[rows(i)] = jnp.dot(x_v[rows(i)], w_v[:, 256:512], preferred_element_type=jnp.float32).astype(jnp.bfloat16)
        return carry

    lax.fori_loop(0, NCHUNK, project_q, 0)

    for j in range(1, HALF + 1):
        for p in (K, V):
            if (p, j) in up_ref:
                @pl.when(up_arrives(p, j, z))
                def _():
                    up_copy(p, j).wait_recv()
                    send_up(p, j + 1)
                    spread(j, p, up_ref[p, j], z - j, True)
            if (p, j) in dn_ref:
                @pl.when(dn_arrives(p, j, z))
                def _():
                    dn_copy(p, j).wait_recv()
                    send_down(p, j + 1)

                    @pl.when(z + j >= NZ)
                    def _():
                        spread(HALF + j, p, dn_ref[p, j], z + j - NZ, True)
        if j == 2:
            for i in (0, 1):
                wy(*y_recvs[i]).wait_recv()
                wy(*y_sends[2 + i]).start()
                wd(*d_sends[1 + i]).start()
        if j == HALF:
            for i in (2, 3):
                wy(*y_recvs[i]).wait_recv()
                wd(*d_sends[1 + i]).start()

    def each_x(act):
        for p in (K, V):
            for d in range(1, NX):
                act(0, p, d, z, None)
                for j in range(1, HALF + 1):
                    if (p, j) in up_ref:
                        act(j, p, d, z - j, z - j >= 0)
                    if (p, j) in dn_ref:
                        act(HALF + j, p, d, z + j - NZ, z + j >= NZ)

    def wait_x(a, p, d, source, when):
        sender = (x + NX - d) % NX

        @pl.when(sender < x if when is None else when)
        def _():
            x_copy(a, p, d, source, sender).wait_recv()

    each_x(wait_x)

    far_count = jnp.minimum(kv, NFAR)
    row_at = lax.broadcasted_iota(jnp.int32, (2 * SPAN, LISTED), 0) & (SPAN - 1)
    col_at = lax.broadcasted_iota(jnp.int32, (2 * SPAN, LISTED), 1)
    last_at = jnp.where(col_at < SPAN, row_at, SPAN - 1 + far_count * KSPAN)

    def att_copy(b, sender):
        return pltpu.make_async_remote_copy(
            src_ref=att.at[b], dst_ref=att_all.at[sender], send_sem=att_send.at[b], recv_sem=att_recv.at[sender],
            device_id=at_tp(b), device_id_type=MESH,
        )

    def attend(i, carry):
        b = (tp + 1 + i) % TP
        kb[0:SPAN] = own_k[pl.ds(b * (SPAN // KSPAN), SPAN // KSPAN)].reshape(SPAN, HEAD)
        vb[0:SPAN] = own_v[pl.ds(b * (SPAN // KSPAN), SPAN // KSPAN)].reshape(SPAN, HEAD)
        for j in range(NFAR):
            picked = jnp.maximum(chosen_s[b, j], 0)
            at = (picked >> 5) * NQB + b
            kb[SPAN + j * KSPAN : SPAN + (j + 1) * KSPAN] = uni_k[at]
            block = uni_v[at]
            vb[SPAN + j * KSPAN : SPAN + (j + 1) * KSPAN] = jnp.where(j < far_count, block, jnp.zeros_like(block))
        q_rows = pl.ds(pl.multiple_of(b * SPAN, SPAN), SPAN)
        qs = jnp.concatenate([q_v[q_rows, 0:HEAD], q_v[q_rows, HEAD:QW]], axis=0)
        scores = lax.dot_general(qs, kb[...], (((1,), (1,)), ((), ())), preferred_element_type=jnp.float32) * SCALE
        scores = jnp.where(col_at <= last_at, scores, -jnp.inf)
        top = jnp.max(scores, axis=1, keepdims=True)
        grown = jnp.exp(scores - top)
        total = jnp.sum(grown, axis=1, keepdims=True)
        weights = (grown * (1.0 / total)).astype(jnp.bfloat16)
        mixed = jnp.dot(weights, vb[...], preferred_element_type=jnp.float32).astype(jnp.bfloat16)
        joined = jnp.concatenate([mixed[:SPAN], mixed[SPAN:]], axis=1)

        @pl.when(i < TP - 1)
        def _():
            att[b] = joined
            att_copy(b, tp).start()

        @pl.when(i == TP - 1)
        def _():
            att_all[tp] = joined

        return carry

    lax.fori_loop(0, TP, attend, 0)

    for args in d_recvs:
        wd(*args).wait_recv()

    def gather(i, carry):
        g = (tp + TP - 1 - i) % TP

        @pl.when(i < TP - 1)
        def _():
            att_copy(tp, g).wait_recv()

        part = jnp.dot(att_all[g], wfull[g], preferred_element_type=jnp.float32).astype(jnp.bfloat16).astype(jnp.float32)

        @pl.when(i == 0)
        def _():
            acc[...] = part

        @pl.when(i > 0)
        def _():
            acc[...] += part

        return carry

    lax.fori_loop(0, TP, gather, 0)
    out_ref[...] = acc[...].astype(jnp.bfloat16)

    for d in range(1, NX):
        tab_copy(d).wait_send()
    for args in y_sends:
        wy(*args).wait_send()
    for args in d_sends:
        wd(*args).wait_send()
    for (p, j) in up_ref:
        @pl.when(up_arrives(p, j, z + 1))
        def _():
            up_copy(p, j).wait_send()
    for (p, j) in dn_ref:
        @pl.when(dn_arrives(p, j, (z + NZ - 1) % NZ))
        def _():
            dn_copy(p, j).wait_send()

    def wait_sent(a, p, d, source, when):
        @pl.when(x + d < NX if when is None else when)
        def _():
            x_copy(a, p, d, source, x).wait_send()

    each_x(wait_sent)

    def att_sent(i, carry):
        b = (tp + 1 + i) % TP
        att_copy(b, tp).wait_send()
        return carry

    lax.fori_loop(0, TP - 1, att_sent, 0)


def shards(tokens, query_weight, key_projection_matrix, value_projection_matrix, out_weight, chosen):
    bf16 = jnp.bfloat16
    piece = pltpu.VMEM((NBLK, KSPAN, HEAD), bf16)
    dma = pltpu.SemaphoreType.DMA
    any_space = pl.BlockSpec(memory_space=pl.ANY)
    arrivals = 2 * HALF + 1
    return pl.pallas_call(
        kernel,
        out_shape=jax.ShapeDtypeStruct((SPAN, WIDTH), bf16),
        in_specs=[any_space] * 5 + [pl.BlockSpec(memory_space=pltpu.VMEM), pl.BlockSpec(memory_space=pltpu.SMEM)],
        out_specs=pl.BlockSpec(memory_space=pltpu.VMEM),
        scratch_shapes=[
            pltpu.VMEM((TOK, WIDTH), bf16),
            pltpu.VMEM((WIDTH, 2 * HEAD + QW), bf16),
            pltpu.VMEM((TP, QW, WIDTH), bf16),
            pltpu.VMEM((TOK, QW), bf16),
            piece,
            piece,
            [piece for _ in UP],
            [piece for _ in DOWN],
            pltpu.VMEM((GROUPS * NQB, KSPAN, HEAD), bf16),
            pltpu.VMEM((GROUPS * NQB, KSPAN, HEAD), bf16),
            pltpu.VMEM((arrivals * 2 * (NX - 1) * NQB, KSPAN, HEAD), bf16),
            pltpu.VMEM((NX, NQB, 128), jnp.int32),
            pltpu.SMEM((NX, NQB, 128), jnp.int32),
            pltpu.VMEM((LISTED, HEAD), bf16),
            pltpu.VMEM((LISTED, HEAD), bf16),
            pltpu.VMEM((TP, SPAN, QW), bf16),
            pltpu.VMEM((TP, SPAN, QW), bf16),
            pltpu.VMEM((SPAN, WIDTH), jnp.float32),
            dma((NCHUNK,)), dma((3,)), dma((1,)), dma((NX,)), dma((NX,)), dma((NX,)),
            dma((2, HALF + 1)), dma((2, HALF + 1)), dma((2, HALF + 1)), dma((2, HALF + 1)),
            dma((arrivals, 2, NX - 1)), dma((arrivals, 2, NX - 1)),
            dma((4,)), dma((4,)), dma((5,)), dma((5,)), dma((TP,)), dma((TP,)),
        ],
        compiler_params=pltpu.CompilerParams(
            collective_id=0, has_side_effects=True, vmem_limit_bytes=56 * 2**20
        ),
        name="sparse_attention_layer",
    )(tokens, query_weight, key_projection_matrix, value_projection_matrix, out_weight, chosen, chosen)


def solution(mesh):
    return jax.shard_map(
        shards,
        mesh=mesh,
        in_specs=(
            P("kv", None),
            P(None, "tp"),
            P(None, "tp"),
            P(None, "tp"),
            P("tp", None),
            P("kv", None),
        ),
        out_specs=P(("kv", "tp"), None),
        check_vma=False,
    )
```

```python
import functools

import jax
import jax.numpy as jnp
from jax import lax
from jax.experimental import pallas as pl
from jax.experimental.pallas import tpu as pltpu
from jax.sharding import PartitionSpec as P

MESH = pl.DeviceIdType.MESH
NZ, NX, NY, NC = 8, 4, 4, 2
TP = NY * NC
HALF = NZ // 2
HEAD = 128
SPAN = 128
KSPAN = 32
NFAR = 12
TOK = 1024
NBLK = TOK // KSPAN
NQB = TOK // SPAN
WIDTH = 2048
QW = 256
GROUPS = NZ * NX
LISTED = SPAN + NFAR * KSPAN
CHUNK = 256
NCHUNK = TOK // CHUNK
LOG_SCALE = HEAD ** (-0.5) * 1.4426950408889634
K, V = 0, 1
UP = [(p, j) for j in range(1, HALF) for p in (K, V)]
DOWN = [(K, j) for j in range(1, HALF)] + [(V, j) for j in range(1, HALF + 1)]
LAST = NZ - 1


def kernel(
    tok_h, wq_h, wk_h, wv_h, wo_h, chosen_h,
    out_ref,
    chosen_v, chosen_s, chosen_sem,
    x_v, w_v, wfull, q_v, own_k, own_v, up_bufs, dn_bufs, uni_k, uni_v, stage, relay_bufs, relay_stage,
    tab_v, tab_s, kb, vb, att, att_all, acc,
    tok_sem, w_sem, wo_sem, tab_send, tab_recv, tab_loc,
    up_send, up_recv, dn_send, dn_recv, x_send, x_recv, r_send, r_recv,
    wy_send, wy_recv, wd_send, wd_recv, att_send, att_recv,
):
    kv = lax.axis_index("kv")
    tp = lax.axis_index("tp")
    z, x = kv // NX, kv % NX
    y, c = tp // NC, tp % NC

    def at_z(step):
        return {"kv": ((z + step + NZ) % NZ) * NX + x, "tp": tp}

    def at_x(step):
        return {"kv": z * NX + (x + step + NX) % NX, "tp": tp}

    def at_zx(dz, dx):
        return {"kv": ((z + dz + NZ) % NZ) * NX + (x + dx) % NX, "tp": tp}

    def at_tp(index):
        return {"kv": kv, "tp": index}

    def tp_of(dy, dc):
        return ((y + dy + NY) % NY) * NC + (c + dc) % NC

    bar = pltpu.get_barrier_semaphore()
    for dev in [at_zx(dz, d) for dz in (1, -1) for d in range(NX)] + [at_x(d) for d in range(1, NX)]:
        pl.semaphore_signal(bar, inc=1, device_id=dev, device_id_type=MESH)
    for d in range(1, TP):
        pl.semaphore_signal(bar, inc=1, device_id=at_tp((tp + d) % TP), device_id_type=MESH)

    listed_copies = [
        pltpu.make_async_copy(chosen_h, chosen_v, chosen_sem.at[0]),
        pltpu.make_async_copy(chosen_h, chosen_s, chosen_sem.at[1]),
    ]
    for copy in listed_copies:
        copy.start()

    def rows(i):
        return pl.ds(pl.multiple_of(i * CHUNK, CHUNK), CHUNK)

    def tok_copy(i):
        return pltpu.make_async_copy(tok_h.at[rows(i)], x_v.at[rows(i)], tok_sem.at[i])

    w_copies = [
        pltpu.make_async_copy(wk_h, w_v.at[:, 0:128], w_sem.at[0]),
        pltpu.make_async_copy(wv_h, w_v.at[:, 128:256], w_sem.at[1]),
        pltpu.make_async_copy(wq_h, w_v.at[:, 256:512], w_sem.at[2]),
    ]
    w_copies[0].start()
    w_copies[1].start()
    for i in range(NCHUNK):
        tok_copy(i).start()
    wo_copy = pltpu.make_async_copy(wo_h, wfull.at[tp], wo_sem.at[0])
    wo_copy.start()
    w_copies[2].start()

    lane = lax.broadcasted_iota(jnp.int32, (NQB, 128), 1)
    table = jnp.zeros((NQB, 128), jnp.int32)
    for copy in listed_copies:
        copy.wait()
    listed = chosen_v[...]
    for j in range(NFAR):
        col = jnp.broadcast_to(listed[:, j : j + 1], (NQB, 128))
        table = table + jnp.where((col >= 0) & ((col >> 5) == lane), col & (NBLK - 1), 0)
    tab_v[0] = table

    w_copies[0].wait()
    w_copies[1].wait()

    def project_kv(i, carry):
        tok_copy(i).wait()
        pair = jnp.dot(x_v[rows(i)], w_v[:, 0:256], preferred_element_type=jnp.float32).astype(jnp.bfloat16)
        blocks = pl.ds(i * (CHUNK // KSPAN), CHUNK // KSPAN)
        own_k[blocks] = pair[:, :HEAD].reshape(CHUNK // KSPAN, KSPAN, HEAD)
        own_v[blocks] = pair[:, HEAD:].reshape(CHUNK // KSPAN, KSPAN, HEAD)
        return carry

    lax.fori_loop(0, NCHUNK, project_kv, 0)

    pl.semaphore_wait(bar, 2 * NX + NX - 1 + TP - 1)

    def tab_copy(d):
        return pltpu.make_async_remote_copy(
            src_ref=tab_v.at[0], dst_ref=tab_v.at[d], send_sem=tab_send.at[d], recv_sem=tab_recv.at[d],
            device_id=at_x(d), device_id_type=MESH,
        )

    def tab_to_smem(d):
        return pltpu.make_async_copy(tab_v.at[d], tab_s.at[d], tab_loc.at[d])

    def tab_relay_copy(d, dz):
        return pltpu.make_async_remote_copy(
            src_ref=tab_v.at[0], dst_ref=tab_v.at[NX + d], send_sem=tab_send.at[NX * (1 if dz < 0 else 2) + d],
            recv_sem=tab_recv.at[NX + d], device_id=at_zx(dz, d), device_id_type=MESH,
        )

    relays = (z == 0) | ((z >= HALF - 2) & (z <= LAST - 1))
    for d in range(1, NX):
        tab_copy(d).start()

    @pl.when(z >= HALF - 1)
    def _():
        for d in range(NX):
            tab_relay_copy(d, -1).start()

    @pl.when(z == LAST)
    def _():
        for d in range(NX):
            tab_relay_copy(d, 1).start()

    tab_to_smem(0).start()

    def wy(slot, sem, dy, lo, hi):
        ref = wfull.at[slot, lo:hi]
        return pltpu.make_async_remote_copy(
            src_ref=ref, dst_ref=ref, send_sem=wy_send.at[sem], recv_sem=wy_recv.at[sem],
            device_id=at_tp(tp_of(dy, 0)), device_id_type=MESH,
        )

    def wd(slot, sem, lo, hi):
        ref = wfull.at[slot, lo:hi]
        return pltpu.make_async_remote_copy(
            src_ref=ref, dst_ref=ref, send_sem=wd_send.at[sem], recv_sem=wd_recv.at[sem],
            device_id=at_tp(tp_of(0, 1)), device_id_type=MESH,
        )

    y_sends = [(tp, 0, 1, 0, QW), (tp, 1, -1, 0, QW), (tp_of(-1, 0), 2, 1, 0, QW // 2), (tp_of(1, 0), 3, -1, QW // 2, QW)]
    y_recvs = [
        (tp_of(-1, 0), 0, 1, 0, QW), (tp_of(1, 0), 1, -1, 0, QW),
        (tp_of(2, 0), 2, 1, 0, QW // 2), (tp_of(2, 0), 3, -1, QW // 2, QW),
    ]
    d_rows = [(0, QW), (0, QW), (0, QW), (0, QW // 2), (QW // 2, QW)]
    d_sends = [(s, i) + d_rows[i] for i, s in enumerate([tp, tp_of(-1, 0), tp_of(1, 0), tp_of(2, 0), tp_of(2, 0)])]
    d_recvs = [(s, i) + d_rows[i] for i, s in enumerate([tp_of(0, 1), tp_of(-1, 1), tp_of(1, 1), tp_of(2, 1), tp_of(2, 1)])]
    wo_copy.wait()
    wy(*y_sends[0]).start()
    wy(*y_sends[1]).start()
    wd(*d_sends[0]).start()

    own = {K: own_k, V: own_v}
    up_ref = {(p, j): up_bufs[i] for i, (p, j) in enumerate(UP)}
    dn_ref = {(p, j): dn_bufs[i] for i, (p, j) in enumerate(DOWN)}
    uni = {K: uni_k, V: uni_v}

    def up_copy(p, j):
        src = own[p] if j == 1 else up_ref[p, j - 1]
        return pltpu.make_async_remote_copy(
            src_ref=src, dst_ref=up_ref[p, j], send_sem=up_send.at[p, j], recv_sem=up_recv.at[p, j],
            device_id=at_z(1), device_id_type=MESH,
        )

    def dn_copy(p, j):
        src = own[p] if j == 1 else dn_ref[p, j - 1]
        return pltpu.make_async_remote_copy(
            src_ref=src, dst_ref=dn_ref[p, j], send_sem=dn_send.at[p, j], recv_sem=dn_recv.at[p, j],
            device_id=at_z(-1), device_id_type=MESH,
        )

    def up_arrives(p, j, here):
        first = LAST if (p, j) == (V, HALF - 1) else j
        return (here >= first) & (here <= LAST)

    def dn_arrives(p, j, here):
        source = (here + j) % NZ
        lands = source <= (HALF - 2 if p == K else HALF - 1)
        if (p, j) in ((K, HALF - 1), (V, HALF)):
            lands = lands & (here != LAST)
        return lands

    def send_up(p, j):
        if (p, j) in up_ref:
            @pl.when(up_arrives(p, j, z + 1))
            def _():
                up_copy(p, j).start()

    def send_down(p, j):
        if (p, j) in dn_ref:
            @pl.when(dn_arrives(p, j, (z + NZ - 1) % NZ))
            def _():
                dn_copy(p, j).start()

    RELAYS = [
        (0, V, HALF - 2, 1, HALF - 2, LAST - 2),
        (1, K, HALF - 1, 1, HALF - 1, LAST - 1),
        (0, K, HALF - 2, -1, 0, 0),
        (1, V, HALF - 1, -1, 0, 0),
    ]

    def relay_x_copy(slot, d, sender_x):
        return pltpu.make_async_remote_copy(
            src_ref=relay_stage.at[slot * (NX - 1) + d - 1], dst_ref=relay_bufs[slot].at[sender_x],
            send_sem=r_send.at[slot, d], recv_sem=r_recv.at[slot, d],
            device_id=at_x(d), device_id_type=MESH,
        )

    def relay_z_copy(slot, p, j, dz, source):
        sems = (up_send, up_recv) if dz == 1 else (dn_send, dn_recv)
        return pltpu.make_async_remote_copy(
            src_ref=relay_bufs[slot], dst_ref=uni[p].at[pl.ds(source * NX, NX)],
            send_sem=sems[0].at[p, j], recv_sem=sems[1].at[p, j],
            device_id=at_z(dz), device_id_type=MESH,
        )

    def relay_begin(slot, p, buf, source):
        group = source * NX + x

        def pick(i, carry):
            b = (tp + 1 + i) % TP
            for d in range(NX):
                block = buf[tab_s[NX + (NX - d) % NX, b, group]]
                if d == 0:
                    relay_bufs[slot][x, i] = block
                else:
                    relay_stage[slot * (NX - 1) + d - 1, i] = block
            return carry

        lax.fori_loop(0, NQB, pick, 0)
        for d in range(1, NX):
            relay_x_copy(slot, d, x).start()

    def relay_end(slot, p, j, dz, source):
        for d in range(1, NX):
            relay_x_copy(slot, d, (x + NX - d) % NX).wait_recv()
        relay_z_copy(slot, p, j + 1, dz, source).start()

    def relay_for(p, j, dz):
        for slot, rp, rj, rdz, low, high in RELAYS:
            if (rp, rj, rdz) == (p, j, dz):
                return slot, (z >= low) & (z <= high)
        return None

    def stage_at(a, p, d):
        return (a * 2 + p) * (NX - 1) + d - 1

    def x_copy(a, p, d, source, sender_x):
        return pltpu.make_async_remote_copy(
            src_ref=stage.at[stage_at(a, p, d)],
            dst_ref=uni[p].at[source * NX + sender_x],
            send_sem=x_send.at[a, p, d - 1], recv_sem=x_recv.at[a, p, d - 1],
            device_id=at_x(d), device_id_type=MESH,
        )

    def spread(a, p, buf, source, mine):
        group = source * NX + x

        def pick(i, carry):
            b = (tp + 1 + i) % TP
            for d in range(1, NX):
                stage[stage_at(a, p, d), i] = buf[tab_s[NX - d, b, group]]
            if mine:
                uni[p][group, i] = buf[tab_s[0, b, group]]
            return carry

        lax.fori_loop(0, NQB, pick, 0)
        for d in range(1, NX):
            if mine:
                x_copy(a, p, d, source, x).start()
            else:
                @pl.when(x + d < NX)
                def _():
                    x_copy(a, p, d, source, x).start()

    for p in (K, V):
        send_up(p, 1)
        send_down(p, 1)

    for d in range(1, NX):
        tab_copy(d).wait_recv()
        tab_to_smem(d).start()
    for d in range(NX):
        tab_to_smem(d).wait()

    @pl.when(relays)
    def _():
        for d in range(NX):
            tab_relay_copy(d, -1).wait_recv()
            tab_to_smem(NX + d).start()
        for d in range(NX):
            tab_to_smem(NX + d).wait()

    spread(0, K, own_k, z, False)
    spread(0, V, own_v, z, False)

    w_copies[2].wait()

    def project_q(i, carry):
        q_v[rows(i)] = jnp.dot(x_v[rows(i)], w_v[:, 256:512], preferred_element_type=jnp.float32).astype(jnp.bfloat16)
        return carry

    lax.fori_loop(0, NCHUNK, project_q, 0)

    for j in range(1, HALF + 1):
        for p in (K, V):
            if (p, j) in up_ref:
                @pl.when(up_arrives(p, j, z))
                def _():
                    up_copy(p, j).wait_recv()
                    send_up(p, j + 1)
                    found = relay_for(p, j, 1)
                    if found:
                        @pl.when(found[1])
                        def _():
                            relay_begin(found[0], p, up_ref[p, j], z - j)
                    spread(j, p, up_ref[p, j], z - j, True)
            if (p, j) in dn_ref:
                @pl.when(dn_arrives(p, j, z))
                def _():
                    dn_copy(p, j).wait_recv()
                    send_down(p, j + 1)
                    found = relay_for(p, j, -1)
                    if found:
                        @pl.when(found[1])
                        def _():
                            relay_begin(found[0], p, dn_ref[p, j], z + j)

                    @pl.when(z + j >= NZ)
                    def _():
                        spread(HALF + j, p, dn_ref[p, j], z + j - NZ, True)
        for slot, p, rj, dz, low, high in RELAYS:
            if rj == j:
                @pl.when((z >= low) & (z <= high))
                def _():
                    relay_end(slot, p, rj, dz, z - rj if dz == 1 else z + rj)
        if j == 2:
            for i in (0, 1):
                wy(*y_recvs[i]).wait_recv()
                wy(*y_sends[2 + i]).start()
                wd(*d_sends[1 + i]).start()
        if j == HALF:
            for i in (2, 3):
                wy(*y_recvs[i]).wait_recv()
                wd(*d_sends[1 + i]).start()

    divided = [
        (0, V, HALF - 1, 1, (z >= HALF - 1) & (z <= LAST - 1)),
        (1, K, HALF, 1, z >= HALF),
        (0, K, HALF - 1, -1, z == LAST),
        (1, V, HALF, -1, z == LAST),
    ]
    for slot, p, j, dz, when in divided:
        @pl.when(when)
        def _():
            relay_z_copy(slot, p, j, dz, z - j if dz == 1 else z + j - NZ).wait_recv()

    def each_x(act):
        for p in (K, V):
            for d in range(1, NX):
                act(0, p, d, z, None)
                for j in range(1, HALF + 1):
                    if (p, j) in up_ref:
                        act(j, p, d, z - j, up_arrives(p, j, z))
                    if (p, j) in dn_ref:
                        act(HALF + j, p, d, z + j - NZ, dn_arrives(p, j, z) & (z + j >= NZ))

    def wait_x(a, p, d, source, when):
        sender = (x + NX - d) % NX

        @pl.when(sender < x if when is None else when)
        def _():
            x_copy(a, p, d, source, sender).wait_recv()

    each_x(wait_x)

    far_count = jnp.minimum(kv, NFAR)
    near_row = lax.broadcasted_iota(jnp.int32, (2 * SPAN, SPAN), 0) & (SPAN - 1)
    near_col = lax.broadcasted_iota(jnp.int32, (2 * SPAN, SPAN), 1)
    far_col = lax.broadcasted_iota(jnp.int32, (2 * SPAN, NFAR * KSPAN), 1)

    def att_copy(b, sender):
        return pltpu.make_async_remote_copy(
            src_ref=att.at[b], dst_ref=att_all.at[sender], send_sem=att_send.at[b], recv_sem=att_recv.at[sender],
            device_id=at_tp(b), device_id_type=MESH,
        )

    def attend_block(i, kb, vb):
        b = (tp + 1 + i) % TP
        kb[0:SPAN] = own_k[pl.ds(b * (SPAN // KSPAN), SPAN // KSPAN)].reshape(SPAN, HEAD)
        vb[0:SPAN] = own_v[pl.ds(b * (SPAN // KSPAN), SPAN // KSPAN)].reshape(SPAN, HEAD)
        for j in range(NFAR):
            picked = jnp.maximum(chosen_s[b, j], 0)
            kb[SPAN + j * KSPAN : SPAN + (j + 1) * KSPAN] = uni_k[picked >> 5, i]
            block = uni_v[picked >> 5, i]
            vb[SPAN + j * KSPAN : SPAN + (j + 1) * KSPAN] = jnp.where(j < far_count, block, jnp.zeros_like(block))
        q_rows = pl.ds(pl.multiple_of(b * SPAN, SPAN), SPAN)
        qs = jnp.concatenate([q_v[q_rows, 0:HEAD], q_v[q_rows, HEAD:QW]], axis=0)
        scores = lax.dot_general(qs, kb[...], (((1,), (1,)), ((), ())), preferred_element_type=jnp.float32)
        near = jnp.where(near_col <= near_row, scores[:, :SPAN], -jnp.inf)
        far = jnp.where(far_col < far_count * KSPAN, scores[:, SPAN:], -jnp.inf)
        scores = jnp.concatenate([near, far], axis=1) * LOG_SCALE
        top = jnp.max(scores, axis=1, keepdims=True)
        grown = jnp.exp2(scores - top)
        total = jnp.sum(grown, axis=1, keepdims=True)
        weights = (grown * (1.0 / total)).astype(jnp.bfloat16)
        mixed = jnp.dot(weights, vb[...], preferred_element_type=jnp.float32).astype(jnp.bfloat16)
        return jnp.concatenate([mixed[:SPAN], mixed[SPAN:]], axis=1)

    def attend(i, carry):
        first, second = (tp + 1 + 2 * i) % TP, (tp + 2 + 2 * i) % TP
        one = attend_block(2 * i, kb.at[0], vb.at[0])
        two = attend_block(2 * i + 1, kb.at[1], vb.at[1])
        att[first] = one
        att[second] = two
        att_copy(first, tp).start()

        @pl.when(i < TP // 2 - 1)
        def _():
            att_copy(second, tp).start()

        return carry

    lax.fori_loop(0, TP // 2, attend, 0)

    for args in d_recvs:
        wd(*args).wait_recv()

    def part_of(piece, g):
        return jnp.dot(piece, wfull[g], preferred_element_type=jnp.float32).astype(jnp.bfloat16).astype(jnp.float32)

    def gather(i, carry):
        g, h = (tp + TP - 1 - 2 * i) % TP, (tp + TP - 2 - 2 * i) % TP
        att_copy(tp, g).wait_recv()
        att_copy(tp, h).wait_recv()
        acc[...] += part_of(att_all[g], g) + part_of(att_all[h], h)
        return carry

    acc[...] = part_of(att[tp], tp)
    lax.fori_loop(0, TP // 2 - 1, gather, 0)
    last = (tp + 1) % TP
    att_copy(tp, last).wait_recv()
    out_ref[...] = (acc[...] + part_of(att_all[last], last)).astype(jnp.bfloat16)

    for d in range(1, NX):
        tab_copy(d).wait_send()

    @pl.when(z >= HALF - 1)
    def _():
        for d in range(NX):
            tab_relay_copy(d, -1).wait_send()

    @pl.when(z == LAST)
    def _():
        for d in range(NX):
            tab_relay_copy(d, 1).wait_send()

    for args in y_sends:
        wy(*args).wait_send()
    for args in d_sends:
        wd(*args).wait_send()
    for (p, j) in up_ref:
        @pl.when(up_arrives(p, j, z + 1))
        def _():
            up_copy(p, j).wait_send()
    for (p, j) in dn_ref:
        @pl.when(dn_arrives(p, j, (z + NZ - 1) % NZ))
        def _():
            dn_copy(p, j).wait_send()

    for slot, p, rj, dz, low, high in RELAYS:
        @pl.when((z >= low) & (z <= high))
        def _():
            for d in range(1, NX):
                relay_x_copy(slot, d, x).wait_send()
            relay_z_copy(slot, p, rj + 1, dz, z - rj if dz == 1 else z + rj).wait_send()

    def wait_sent(a, p, d, source, when):
        @pl.when(x + d < NX if when is None else when)
        def _():
            x_copy(a, p, d, source, x).wait_send()

    each_x(wait_sent)

    def att_sent(i, carry):
        b = (tp + 1 + i) % TP
        att_copy(b, tp).wait_send()
        return carry

    lax.fori_loop(0, TP - 1, att_sent, 0)


def shards(tokens, query_weight, key_projection_matrix, value_projection_matrix, out_weight, chosen):
    bf16 = jnp.bfloat16
    piece = pltpu.VMEM((NBLK, KSPAN, HEAD), bf16)
    dma = pltpu.SemaphoreType.DMA
    any_space = pl.BlockSpec(memory_space=pl.ANY)
    arrivals = 2 * HALF + 1
    return pl.pallas_call(
        kernel,
        out_shape=jax.ShapeDtypeStruct((SPAN, WIDTH), bf16),
        in_specs=[any_space] * 6,
        out_specs=pl.BlockSpec(memory_space=pltpu.VMEM),
        scratch_shapes=[
            pltpu.VMEM((NQB, NFAR), jnp.int32),
            pltpu.SMEM((NQB, NFAR), jnp.int32),
            dma((2,)),
            pltpu.VMEM((TOK, WIDTH), bf16),
            pltpu.VMEM((WIDTH, 2 * HEAD + QW), bf16),
            pltpu.VMEM((TP, QW, WIDTH), bf16),
            pltpu.VMEM((TOK, QW), bf16),
            piece,
            piece,
            [piece for _ in UP],
            [piece for _ in DOWN],
            pltpu.VMEM((GROUPS, NQB, KSPAN, HEAD), bf16),
            pltpu.VMEM((GROUPS, NQB, KSPAN, HEAD), bf16),
            pltpu.VMEM((arrivals * 2 * (NX - 1), NQB, KSPAN, HEAD), bf16),
            [pltpu.VMEM((NX, NQB, KSPAN, HEAD), bf16) for _ in range(2)],
            pltpu.VMEM((2 * (NX - 1), NQB, KSPAN, HEAD), bf16),
            pltpu.VMEM((2 * NX, NQB, 128), jnp.int32),
            pltpu.SMEM((2 * NX, NQB, 128), jnp.int32),
            pltpu.VMEM((2, LISTED, HEAD), bf16),
            pltpu.VMEM((2, LISTED, HEAD), bf16),
            pltpu.VMEM((TP, SPAN, QW), bf16),
            pltpu.VMEM((TP, SPAN, QW), bf16),
            pltpu.VMEM((SPAN, WIDTH), jnp.float32),
            dma((NCHUNK,)), dma((3,)), dma((1,)), dma((3 * NX,)), dma((2 * NX,)), dma((2 * NX,)),
            dma((2, HALF + 1)), dma((2, HALF + 1)), dma((2, HALF + 1)), dma((2, HALF + 1)),
            dma((arrivals, 2, NX - 1)), dma((arrivals, 2, NX - 1)), dma((2, NX)), dma((2, NX)),
            dma((4,)), dma((4,)), dma((5,)), dma((5,)), dma((TP,)), dma((TP,)),
        ],
        compiler_params=pltpu.CompilerParams(
            collective_id=0, has_side_effects=True, vmem_limit_bytes=56 * 2**20
        ),
        name="sparse_attention_layer",
    )(tokens, query_weight, key_projection_matrix, value_projection_matrix, out_weight, chosen)


def solution(mesh):
    return jax.shard_map(
        shards,
        mesh=mesh,
        in_specs=(
            P("kv", None),
            P(None, "tp"),
            P(None, "tp"),
            P(None, "tp"),
            P("tp", None),
            P("kv", None),
        ),
        out_specs=P(("kv", "tp"), None),
        check_vma=False,
    )
```

```python
import functools

import jax
import jax.numpy as jnp
from jax import lax
from jax.experimental import pallas as pl
from jax.experimental.pallas import tpu as pltpu
from jax.sharding import PartitionSpec as P

MESH = pl.DeviceIdType.MESH
NZ, NX, NY, NC = 8, 4, 4, 2
TP = NY * NC
HALF = NZ // 2
HEAD = 128
SPAN = 128
KSPAN = 32
NFAR = 12
TOK = 1024
NBLK = TOK // KSPAN
NQB = TOK // SPAN
WIDTH = 2048
QW = 256
GROUPS = NZ * NX
LISTED = SPAN + NFAR * KSPAN
CHUNK = 256
NCHUNK = TOK // CHUNK
LOG_SCALE = HEAD ** (-0.5) * 1.4426950408889634
K, V = 0, 1
UP = [(p, j) for j in range(1, HALF) for p in (K, V)]
DOWN = [(K, j) for j in range(1, HALF)] + [(V, j) for j in range(1, HALF + 1)]
LAST = NZ - 1
LATE = {(HALF - 1, K): 0, (HALF - 1, V): 1, (2 * HALF - 1, K): 2, (2 * HALF, V): 3}
FIRST = NQB // 2


def kernel(
    tok_h, wq_h, wk_h, wv_h, wo_h, chosen_h,
    out_ref,
    chosen_v, chosen_s, chosen_sem,
    x_v, w_v, wfull, q_v, own_k, own_v, up_bufs, dn_bufs, uni_k, uni_v, stage, relay_bufs, relay_stage, late_x, late_relay,
    tab_v, tab_s, kb, vb, att, att_all, acc,
    tok_sem, w_sem, wo_sem, tab_send, tab_recv, tab_loc,
    up_send, up_recv, dn_send, dn_recv, x_send, x_recv, xl_send, xl_recv, r_send, r_recv, rl_send, rl_recv,
    wy_send, wy_recv, wd_send, wd_recv, att_send, att_recv,
):
    kv = lax.axis_index("kv")
    tp = lax.axis_index("tp")
    z, x = kv // NX, kv % NX
    y, c = tp // NC, tp % NC

    def at_z(step):
        return {"kv": ((z + step + NZ) % NZ) * NX + x, "tp": tp}

    def at_x(step):
        return {"kv": z * NX + (x + step + NX) % NX, "tp": tp}

    def at_zx(dz, dx):
        return {"kv": ((z + dz + NZ) % NZ) * NX + (x + dx) % NX, "tp": tp}

    def at_tp(index):
        return {"kv": kv, "tp": index}

    def tp_of(dy, dc):
        return ((y + dy + NY) % NY) * NC + (c + dc) % NC

    def block_at(i, way):
        r, k = i // 2, i % 2
        dy = 2 - (r + 1) // 2
        dy = dy + k * (NY - 2 * dy)
        dc = r // 2 + k * ((r + 1) % 2 - r // 2)
        return ((y + way * dy + NY) % NY) * NC + (c + dc) % NC

    bar = pltpu.get_barrier_semaphore()
    for dev in [at_zx(dz, d) for dz in (1, -1) for d in range(NX)] + [at_x(d) for d in range(1, NX)]:
        pl.semaphore_signal(bar, inc=1, device_id=dev, device_id_type=MESH)
    for d in range(1, TP):
        pl.semaphore_signal(bar, inc=1, device_id=at_tp((tp + d) % TP), device_id_type=MESH)

    listed_copies = [
        pltpu.make_async_copy(chosen_h, chosen_v, chosen_sem.at[0]),
        pltpu.make_async_copy(chosen_h, chosen_s, chosen_sem.at[1]),
    ]
    for copy in listed_copies:
        copy.start()

    def rows(i):
        return pl.ds(pl.multiple_of(i * CHUNK, CHUNK), CHUNK)

    def tok_copy(i):
        return pltpu.make_async_copy(tok_h.at[rows(i)], x_v.at[rows(i)], tok_sem.at[i])

    w_copies = [
        pltpu.make_async_copy(wk_h, w_v.at[:, 0:128], w_sem.at[0]),
        pltpu.make_async_copy(wv_h, w_v.at[:, 128:256], w_sem.at[1]),
        pltpu.make_async_copy(wq_h, w_v.at[:, 256:512], w_sem.at[2]),
    ]
    w_copies[0].start()
    w_copies[1].start()
    for i in range(NCHUNK):
        tok_copy(i).start()
    wo_copy = pltpu.make_async_copy(wo_h, wfull.at[tp], wo_sem.at[0])
    wo_copy.start()
    w_copies[2].start()

    lane = lax.broadcasted_iota(jnp.int32, (NQB, 128), 1)
    table = jnp.zeros((NQB, 128), jnp.int32)
    for copy in listed_copies:
        copy.wait()
    listed = chosen_v[...]
    for j in range(NFAR):
        col = jnp.broadcast_to(listed[:, j : j + 1], (NQB, 128))
        table = table + jnp.where((col >= 0) & ((col >> 5) == lane), col & (NBLK - 1), 0)
    tab_v[0] = table

    w_copies[0].wait()
    w_copies[1].wait()

    def project_kv(i, carry):
        tok_copy(i).wait()
        pair = jnp.dot(x_v[rows(i)], w_v[:, 0:256], preferred_element_type=jnp.float32).astype(jnp.bfloat16)
        blocks = pl.ds(i * (CHUNK // KSPAN), CHUNK // KSPAN)
        own_k[blocks] = pair[:, :HEAD].reshape(CHUNK // KSPAN, KSPAN, HEAD)
        own_v[blocks] = pair[:, HEAD:].reshape(CHUNK // KSPAN, KSPAN, HEAD)
        return carry

    lax.fori_loop(0, NCHUNK, project_kv, 0)

    pl.semaphore_wait(bar, 2 * NX + NX - 1 + TP - 1)

    def tab_copy(d):
        return pltpu.make_async_remote_copy(
            src_ref=tab_v.at[0], dst_ref=tab_v.at[d], send_sem=tab_send.at[d], recv_sem=tab_recv.at[d],
            device_id=at_x(d), device_id_type=MESH,
        )

    def tab_to_smem(d):
        return pltpu.make_async_copy(tab_v.at[d], tab_s.at[d], tab_loc.at[d])

    def tab_relay_copy(d, dz):
        return pltpu.make_async_remote_copy(
            src_ref=tab_v.at[0], dst_ref=tab_v.at[NX + d], send_sem=tab_send.at[NX * (1 if dz < 0 else 2) + d],
            recv_sem=tab_recv.at[NX + d], device_id=at_zx(dz, d), device_id_type=MESH,
        )

    relays = (z == 0) | ((z >= HALF - 2) & (z <= LAST - 1))
    for d in range(1, NX):
        tab_copy(d).start()

    @pl.when(z >= HALF - 1)
    def _():
        for d in range(NX):
            tab_relay_copy(d, -1).start()

    @pl.when(z == LAST)
    def _():
        for d in range(NX):
            tab_relay_copy(d, 1).start()

    tab_to_smem(0).start()

    def wy(slot, sem, dy, lo, hi):
        ref = wfull.at[slot, lo:hi]
        return pltpu.make_async_remote_copy(
            src_ref=ref, dst_ref=ref, send_sem=wy_send.at[sem], recv_sem=wy_recv.at[sem],
            device_id=at_tp(tp_of(dy, 0)), device_id_type=MESH,
        )

    def wd(slot, sem, lo, hi):
        ref = wfull.at[slot, lo:hi]
        return pltpu.make_async_remote_copy(
            src_ref=ref, dst_ref=ref, send_sem=wd_send.at[sem], recv_sem=wd_recv.at[sem],
            device_id=at_tp(tp_of(0, 1)), device_id_type=MESH,
        )

    y_sends = [(tp, 0, 1, 0, QW), (tp, 1, -1, 0, QW), (tp_of(-1, 0), 2, 1, 0, QW // 2), (tp_of(1, 0), 3, -1, QW // 2, QW)]
    y_recvs = [
        (tp_of(-1, 0), 0, 1, 0, QW), (tp_of(1, 0), 1, -1, 0, QW),
        (tp_of(2, 0), 2, 1, 0, QW // 2), (tp_of(2, 0), 3, -1, QW // 2, QW),
    ]
    d_rows = [(0, QW), (0, QW), (0, QW), (0, QW // 2), (QW // 2, QW)]
    d_sends = [(s, i) + d_rows[i] for i, s in enumerate([tp, tp_of(-1, 0), tp_of(1, 0), tp_of(2, 0), tp_of(2, 0)])]
    d_recvs = [(s, i) + d_rows[i] for i, s in enumerate([tp_of(0, 1), tp_of(-1, 1), tp_of(1, 1), tp_of(2, 1), tp_of(2, 1)])]
    wo_copy.wait()
    wy(*y_sends[0]).start()
    wy(*y_sends[1]).start()
    wd(*d_sends[0]).start()

    own = {K: own_k, V: own_v}
    up_ref = {(p, j): up_bufs[i] for i, (p, j) in enumerate(UP)}
    dn_ref = {(p, j): dn_bufs[i] for i, (p, j) in enumerate(DOWN)}
    uni = {K: uni_k, V: uni_v}

    def up_copy(p, j):
        src = own[p] if j == 1 else up_ref[p, j - 1]
        return pltpu.make_async_remote_copy(
            src_ref=src, dst_ref=up_ref[p, j], send_sem=up_send.at[p, j], recv_sem=up_recv.at[p, j],
            device_id=at_z(1), device_id_type=MESH,
        )

    def dn_copy(p, j):
        src = own[p] if j == 1 else dn_ref[p, j - 1]
        return pltpu.make_async_remote_copy(
            src_ref=src, dst_ref=dn_ref[p, j], send_sem=dn_send.at[p, j], recv_sem=dn_recv.at[p, j],
            device_id=at_z(-1), device_id_type=MESH,
        )

    def up_arrives(p, j, here):
        first = LAST if (p, j) == (V, HALF - 1) else j
        return (here >= first) & (here <= LAST)

    def dn_arrives(p, j, here):
        source = (here + j) % NZ
        lands = source <= (HALF - 2 if p == K else HALF - 1)
        if (p, j) in ((K, HALF - 1), (V, HALF)):
            lands = lands & (here != LAST)
        return lands

    def send_up(p, j):
        if (p, j) in up_ref:
            @pl.when(up_arrives(p, j, z + 1))
            def _():
                up_copy(p, j).start()

    def send_down(p, j):
        if (p, j) in dn_ref:
            @pl.when(dn_arrives(p, j, (z + NZ - 1) % NZ))
            def _():
                dn_copy(p, j).start()

    RELAYS = [
        (0, V, HALF - 2, 1, HALF - 2, LAST - 2),
        (1, K, HALF - 1, 1, HALF - 1, LAST - 1),
        (0, K, HALF - 2, -1, 0, 0),
        (1, V, HALF - 1, -1, 0, 0),
    ]

    def relay_x_copy(slot, d, sender_x):
        return pltpu.make_async_remote_copy(
            src_ref=relay_stage.at[slot * (NX - 1) + d - 1], dst_ref=relay_bufs[slot].at[sender_x],
            send_sem=r_send.at[slot, d], recv_sem=r_recv.at[slot, d],
            device_id=at_x(d), device_id_type=MESH,
        )

    def relay_z_copy(slot, p, j, dz, source, second=False):
        send, recv = (up_send, up_recv) if dz == 1 else (dn_send, dn_recv)
        send, recv = (rl_send.at[p], rl_recv.at[p]) if second else (send.at[p, j], recv.at[p, j])
        part = slice(0, NQB) if slot == 0 else slice(FIRST, NQB) if second else slice(0, FIRST)
        return pltpu.make_async_remote_copy(
            src_ref=relay_bufs[slot].at[:, part],
            dst_ref=late_relay[p] if second else uni[p].at[pl.ds(source * NX, NX), part],
            send_sem=send, recv_sem=recv,
            device_id=at_z(dz), device_id_type=MESH,
        )

    def relay_begin(slot, p, buf, source):
        group = source * NX + x

        def pick(i, carry):
            b = block_at(i, 1)
            for d in range(NX):
                block = buf[tab_s[NX + (NX - d) % NX, b, group]]
                if d == 0:
                    relay_bufs[slot][x, i] = block
                else:
                    relay_stage[slot * (NX - 1) + d - 1, i] = block
            return carry

        lax.fori_loop(0, NQB, pick, 0)
        for d in range(1, NX):
            relay_x_copy(slot, d, x).start()

    def relay_end(slot, p, j, dz, source):
        for d in range(1, NX):
            relay_x_copy(slot, d, (x + NX - d) % NX).wait_recv()
        relay_z_copy(slot, p, j + 1, dz, source).start()
        if slot == 1:
            relay_z_copy(slot, p, j + 1, dz, source, True).start()

    def relay_for(p, j, dz):
        for slot, rp, rj, rdz, low, high in RELAYS:
            if (rp, rj, rdz) == (p, j, dz):
                return slot, (z >= low) & (z <= high)
        return None

    def stage_at(a, p, d):
        return (a * 2 + p) * (NX - 1) + d - 1

    def x_copy(a, p, d, source, sender_x, second=False):
        late = LATE.get((a, p))
        part = slice(0, NQB) if late is None else slice(FIRST, NQB) if second else slice(0, FIRST)
        return pltpu.make_async_remote_copy(
            src_ref=stage.at[stage_at(a, p, d), part],
            dst_ref=late_x[late][d - 1] if second else uni[p].at[source * NX + sender_x, part],
            send_sem=xl_send.at[late, d - 1] if second else x_send.at[a, p, d - 1],
            recv_sem=xl_recv.at[late, d - 1] if second else x_recv.at[a, p, d - 1],
            device_id=at_x(d), device_id_type=MESH,
        )

    def spread(a, p, buf, source, mine):
        group = source * NX + x

        def pick(i, carry):
            b = block_at(i, 1)
            for d in range(1, NX):
                stage[stage_at(a, p, d), i] = buf[tab_s[NX - d, b, group]]
            if mine:
                uni[p][group, i] = buf[tab_s[0, b, group]]
            return carry

        lax.fori_loop(0, NQB, pick, 0)
        for d in range(1, NX):
            if mine:
                x_copy(a, p, d, source, x).start()
            else:
                @pl.when(x + d < NX)
                def _():
                    x_copy(a, p, d, source, x).start()

    def each_x(act, second=False):
        for p in (K, V):
            for d in range(1, NX):
                for a, source, when in [(0, z, None)] + [
                    (j, z - j, up_arrives(p, j, z)) for j in range(1, HALF + 1) if (p, j) in up_ref
                ] + [
                    (HALF + j, z + j - NZ, dn_arrives(p, j, z) & (z + j >= NZ)) for j in range(1, HALF + 1) if (p, j) in dn_ref
                ]:
                    if not second or (a, p) in LATE:
                        act(a, p, d, source, when, second)

    for p in (K, V):
        send_up(p, 1)
        send_down(1 - p, 1)

    for d in range(1, NX):
        tab_copy(d).wait_recv()
        tab_to_smem(d).start()
    for d in range(NX):
        tab_to_smem(d).wait()

    @pl.when(relays)
    def _():
        for d in range(NX):
            tab_relay_copy(d, -1).wait_recv()
            tab_to_smem(NX + d).start()
        for d in range(NX):
            tab_to_smem(NX + d).wait()

    spread(0, K, own_k, z, False)
    spread(0, V, own_v, z, False)

    w_copies[2].wait()

    def project_q(i, carry):
        q_v[rows(i)] = jnp.dot(x_v[rows(i)], w_v[:, 256:512], preferred_element_type=jnp.float32).astype(jnp.bfloat16)
        return carry

    lax.fori_loop(0, NCHUNK, project_q, 0)

    def from_below(p, j):
        if (p, j) not in up_ref:
            return

        @pl.when(up_arrives(p, j, z))
        def _():
            up_copy(p, j).wait_recv()
            send_up(p, j + 1)
            found = relay_for(p, j, 1)
            if found:
                @pl.when(found[1])
                def _():
                    relay_begin(found[0], p, up_ref[p, j], z - j)
            spread(j, p, up_ref[p, j], z - j, True)

    def from_above(p, j):
        if (p, j) not in dn_ref:
            return

        @pl.when(dn_arrives(p, j, z))
        def _():
            dn_copy(p, j).wait_recv()
            send_down(p, j + 1)
            found = relay_for(p, j, -1)
            if found:
                @pl.when(found[1])
                def _():
                    relay_begin(found[0], p, dn_ref[p, j], z + j)

            @pl.when(z + j >= NZ)
            def _():
                spread(HALF + j, p, dn_ref[p, j], z + j - NZ, True)

    def start_second(a, p, d, source, when, second):
        @pl.when(when)
        def _():
            x_copy(a, p, d, source, x, second).start()

    def end_relays(wanted, rows_now):
        for slot, p, j, dz, low, high in RELAYS:
            if slot == wanted:
                @pl.when((z >= low) & (z <= high) & rows_now)
                def _():
                    relay_end(slot, p, j, dz, z - j if dz == 1 else z + j)

    for j in range(1, HALF + 1):
        if j == HALF - 1:
            end_relays(0, z == 0)
        if j == HALF:
            end_relays(1, z == LAST - 1)
        from_above(V, j)
        if j == HALF - 1:
            end_relays(0, z != 0)
        if j == HALF:
            each_x(start_second, True)
            end_relays(1, z != LAST - 1)
        from_below(K, j)
        from_above(K, j)
        from_below(V, j)
        if j == 2:
            for i in (0, 1):
                wy(*y_recvs[i]).wait_recv()
                wy(*y_sends[2 + i]).start()
                wd(*d_sends[1 + i]).start()
        if j == HALF:
            for i in (2, 3):
                wy(*y_recvs[i]).wait_recv()
                wd(*d_sends[1 + i]).start()

    divided = [
        (0, V, HALF - 1, 1, (z >= HALF - 1) & (z <= LAST - 1)),
        (1, K, HALF, 1, z >= HALF),
        (0, K, HALF - 1, -1, z == LAST),
        (1, V, HALF, -1, z == LAST),
    ]
    def wait_divided(second):
        for slot, p, j, dz, when in divided:
            if slot == 1 or not second:
                @pl.when(when)
                def _():
                    relay_z_copy(slot, p, j, dz, z - j if dz == 1 else z + j - NZ, second).wait_recv()

    def wait_x(a, p, d, source, when, second):
        sender = (x + NX - d) % NX

        @pl.when(sender < x if when is None else when)
        def _():
            x_copy(a, p, d, source, sender, second).wait_recv()

    each_x(wait_x)
    wait_divided(False)

    def place_second(a, p, d, source, when, second):
        @pl.when(when)
        def _():
            uni[p][source * NX + (x + NX - d) % NX, FIRST:NQB] = late_x[LATE[a, p]][d - 1][...]

    far_count = jnp.minimum(kv, NFAR)
    near_row = lax.broadcasted_iota(jnp.int32, (2 * SPAN, SPAN), 0) & (SPAN - 1)
    near_col = lax.broadcasted_iota(jnp.int32, (2 * SPAN, SPAN), 1)
    far_col = lax.broadcasted_iota(jnp.int32, (2 * SPAN, NFAR * KSPAN), 1)

    def att_copy(b, sender):
        return pltpu.make_async_remote_copy(
            src_ref=att.at[b], dst_ref=att_all.at[sender], send_sem=att_send.at[b], recv_sem=att_recv.at[sender],
            device_id=at_tp(b), device_id_type=MESH,
        )

    def attend_block(i, kb, vb):
        b = block_at(i, 1)
        kb[0:SPAN] = own_k[pl.ds(b * (SPAN // KSPAN), SPAN // KSPAN)].reshape(SPAN, HEAD)
        vb[0:SPAN] = own_v[pl.ds(b * (SPAN // KSPAN), SPAN // KSPAN)].reshape(SPAN, HEAD)
        for j in range(NFAR):
            picked = jnp.maximum(chosen_s[b, j], 0)
            kb[SPAN + j * KSPAN : SPAN + (j + 1) * KSPAN] = uni_k[picked >> 5, i]
            block = uni_v[picked >> 5, i]
            vb[SPAN + j * KSPAN : SPAN + (j + 1) * KSPAN] = jnp.where(j < far_count, block, jnp.zeros_like(block))
        q_rows = pl.ds(pl.multiple_of(b * SPAN, SPAN), SPAN)
        qs = jnp.concatenate([q_v[q_rows, 0:HEAD], q_v[q_rows, HEAD:QW]], axis=0)
        scores = lax.dot_general(qs, kb[...], (((1,), (1,)), ((), ())), preferred_element_type=jnp.float32)
        near = jnp.where(near_col <= near_row, scores[:, :SPAN], -jnp.inf)
        far = jnp.where(far_col < far_count * KSPAN, scores[:, SPAN:], -jnp.inf)
        scores = jnp.concatenate([near, far], axis=1) * LOG_SCALE
        top = jnp.max(scores, axis=1, keepdims=True)
        grown = jnp.exp2(scores - top)
        total = jnp.sum(grown, axis=1, keepdims=True)
        weights = (grown * (1.0 / total)).astype(jnp.bfloat16)
        mixed = jnp.dot(weights, vb[...], preferred_element_type=jnp.float32).astype(jnp.bfloat16)
        return jnp.concatenate([mixed[:SPAN], mixed[SPAN:]], axis=1)

    def attend(i, carry):
        @pl.when(i == FIRST // 2)
        def _():
            each_x(wait_x, True)
            wait_divided(True)
            each_x(place_second, True)
            for _, p, j, dz, when in divided[1::2]:
                @pl.when(when)
                def _():
                    source = z - j if dz == 1 else z + j - NZ
                    uni[p][pl.ds(source * NX, NX), FIRST:NQB] = late_relay[p][...]

        first, second = block_at(2 * i, 1), block_at(2 * i + 1, 1)
        one = attend_block(2 * i, kb.at[0], vb.at[0])
        two = attend_block(2 * i + 1, kb.at[1], vb.at[1])
        att[first] = one
        att[second] = two
        att_copy(first, tp).start()

        @pl.when(i < TP // 2 - 1)
        def _():
            att_copy(second, tp).start()

        return carry

    lax.fori_loop(0, TP // 2, attend, 0)

    for args in d_recvs:
        wd(*args).wait_recv()

    def part_of(piece, g):
        return jnp.dot(piece, wfull[g], preferred_element_type=jnp.float32).astype(jnp.bfloat16).astype(jnp.float32)

    def gather(i, carry):
        g, h = block_at(2 * i, -1), block_at(2 * i + 1, -1)
        att_copy(tp, g).wait_recv()
        att_copy(tp, h).wait_recv()
        acc[...] += part_of(att_all[g], g) + part_of(att_all[h], h)
        return carry

    acc[...] = part_of(att[tp], tp)
    lax.fori_loop(0, TP // 2 - 1, gather, 0)
    last = block_at(TP - 2, -1)
    att_copy(tp, last).wait_recv()
    out_ref[...] = (acc[...] + part_of(att_all[last], last)).astype(jnp.bfloat16)

    for d in range(1, NX):
        tab_copy(d).wait_send()

    @pl.when(z >= HALF - 1)
    def _():
        for d in range(NX):
            tab_relay_copy(d, -1).wait_send()

    @pl.when(z == LAST)
    def _():
        for d in range(NX):
            tab_relay_copy(d, 1).wait_send()

    for args in y_sends:
        wy(*args).wait_send()
    for args in d_sends:
        wd(*args).wait_send()
    for (p, j) in up_ref:
        @pl.when(up_arrives(p, j, z + 1))
        def _():
            up_copy(p, j).wait_send()
    for (p, j) in dn_ref:
        @pl.when(dn_arrives(p, j, (z + NZ - 1) % NZ))
        def _():
            dn_copy(p, j).wait_send()

    for slot, p, rj, dz, low, high in RELAYS:
        @pl.when((z >= low) & (z <= high))
        def _():
            for d in range(1, NX):
                relay_x_copy(slot, d, x).wait_send()
            relay_z_copy(slot, p, rj + 1, dz, z - rj if dz == 1 else z + rj).wait_send()
            if slot == 1:
                relay_z_copy(slot, p, rj + 1, dz, z - rj if dz == 1 else z + rj, True).wait_send()

    def wait_sent(a, p, d, source, when, second):
        @pl.when(x + d < NX if when is None else when)
        def _():
            x_copy(a, p, d, source, x, second).wait_send()

    each_x(wait_sent)
    each_x(wait_sent, True)

    def att_sent(i, carry):
        b = block_at(i, 1)
        att_copy(b, tp).wait_send()
        return carry

    lax.fori_loop(0, TP - 1, att_sent, 0)


def shards(tokens, query_weight, key_projection_matrix, value_projection_matrix, out_weight, chosen):
    bf16 = jnp.bfloat16
    piece = pltpu.VMEM((NBLK, KSPAN, HEAD), bf16)
    dma = pltpu.SemaphoreType.DMA
    any_space = pl.BlockSpec(memory_space=pl.ANY)
    arrivals = 2 * HALF + 1
    return pl.pallas_call(
        kernel,
        out_shape=pltpu.VMEM((SPAN, WIDTH), bf16),
        in_specs=[any_space] * 6,
        out_specs=pl.BlockSpec(memory_space=pltpu.VMEM),
        scratch_shapes=[
            pltpu.VMEM((NQB, NFAR), jnp.int32),
            pltpu.SMEM((NQB, NFAR), jnp.int32),
            dma((2,)),
            pltpu.VMEM((TOK, WIDTH), bf16),
            pltpu.VMEM((WIDTH, 2 * HEAD + QW), bf16),
            pltpu.VMEM((TP, QW, WIDTH), bf16),
            pltpu.VMEM((TOK, QW), bf16),
            piece,
            piece,
            [piece for _ in UP],
            [piece for _ in DOWN],
            pltpu.VMEM((GROUPS, NQB, KSPAN, HEAD), bf16),
            pltpu.VMEM((GROUPS, NQB, KSPAN, HEAD), bf16),
            pltpu.VMEM((arrivals * 2 * (NX - 1), NQB, KSPAN, HEAD), bf16),
            [pltpu.VMEM((NX, NQB, KSPAN, HEAD), bf16) for _ in range(2)],
            pltpu.VMEM((2 * (NX - 1), NQB, KSPAN, HEAD), bf16),
            [[pltpu.VMEM((FIRST, KSPAN, HEAD), bf16) for _ in range(NX - 1)] for _ in LATE],
            [pltpu.VMEM((NX, FIRST, KSPAN, HEAD), bf16) for _ in range(2)],
            pltpu.VMEM((2 * NX, NQB, 128), jnp.int32),
            pltpu.SMEM((2 * NX, NQB, 128), jnp.int32),
            pltpu.VMEM((2, LISTED, HEAD), bf16),
            pltpu.VMEM((2, LISTED, HEAD), bf16),
            pltpu.VMEM((TP, SPAN, QW), bf16),
            pltpu.VMEM((TP, SPAN, QW), bf16),
            pltpu.VMEM((SPAN, WIDTH), jnp.float32),
            dma((NCHUNK,)), dma((3,)), dma((1,)), dma((3 * NX,)), dma((2 * NX,)), dma((2 * NX,)),
            dma((2, HALF + 1)), dma((2, HALF + 1)), dma((2, HALF + 1)), dma((2, HALF + 1)),
            dma((arrivals, 2, NX - 1)), dma((arrivals, 2, NX - 1)),
            dma((len(LATE), NX - 1)), dma((len(LATE), NX - 1)), dma((2, NX)), dma((2, NX)), dma((2,)), dma((2,)),
            dma((4,)), dma((4,)), dma((5,)), dma((5,)), dma((TP,)), dma((TP,)),
        ],
        compiler_params=pltpu.CompilerParams(
            collective_id=0, has_side_effects=True, vmem_limit_bytes=56 * 2**20
        ),
        name="sparse_attention_layer",
    )(tokens, query_weight, key_projection_matrix, value_projection_matrix, out_weight, chosen)


def solution(mesh):
    return jax.shard_map(
        shards,
        mesh=mesh,
        in_specs=(
            P("kv", None),
            P(None, "tp"),
            P(None, "tp"),
            P(None, "tp"),
            P("tp", None),
            P("kv", None),
        ),
        out_specs=P(("kv", "tp"), None),
        check_vma=False,
    )
```

```python
import functools

import jax
import jax.numpy as jnp
from jax import lax
from jax.experimental import pallas as pl
from jax.experimental.pallas import tpu as pltpu
from jax.sharding import PartitionSpec as P

MESH = pl.DeviceIdType.MESH
NZ, NX, NY, NC = 8, 4, 4, 2
TP = NY * NC
HALF = NZ // 2
HEAD = 128
SPAN = 128
KSPAN = 32
NFAR = 12
TOK = 1024
NBLK = TOK // KSPAN
NQB = TOK // SPAN
WIDTH = 2048
QW = 256
GROUPS = NZ * NX
LISTED = SPAN + NFAR * KSPAN
CHUNK = 256
NCHUNK = TOK // CHUNK
LOG_SCALE = HEAD ** (-0.5) * 1.4426950408889634
K, V = 0, 1
UP = [(p, j) for j in range(1, HALF) for p in (K, V)]
DOWN = [(K, j) for j in range(1, HALF)] + [(V, j) for j in range(1, HALF + 1)]
LAST = NZ - 1
LATE = {(HALF - 1, K): 0, (HALF - 1, V): 1, (2 * HALF - 1, K): 2, (2 * HALF, V): 3}
FIRST = NQB // 2


def kernel(
    tok_h, wq_h, wk_h, wv_h, wo_h, chosen_h,
    out_ref,
    chosen_v, chosen_s, chosen_sem,
    x_v, w_v, wfull, q_v, own_k, own_v, up_bufs, dn_bufs, uni_k, uni_v, stage, relay_bufs, relay_stage, late_x, late_relay,
    tab_v, tab_s, kb, vb, att, att_all, acc,
    tok_sem, w_sem, wo_sem, tab_send, tab_recv, tab_loc,
    up_send, up_recv, dn_send, dn_recv, x_send, x_recv, xl_send, xl_recv, r_send, r_recv, rl_send, rl_recv,
    wy_send, wy_recv, wd_send, wd_recv, att_send, att_recv,
):
    kv = lax.axis_index("kv")
    tp = lax.axis_index("tp")
    z, x = kv // NX, kv % NX
    y, c = tp // NC, tp % NC

    def at_z(step):
        return {"kv": ((z + step + NZ) % NZ) * NX + x, "tp": tp}

    def at_x(step):
        return {"kv": z * NX + (x + step + NX) % NX, "tp": tp}

    def at_zx(dz, dx):
        return {"kv": ((z + dz + NZ) % NZ) * NX + (x + dx) % NX, "tp": tp}

    def at_tp(index):
        return {"kv": kv, "tp": index}

    def tp_of(dy, dc):
        return ((y + dy + NY) % NY) * NC + (c + dc) % NC

    def block_at(i, way):
        r, k = i // 2, i % 2
        dy = 2 - (r + 1) // 2
        dy = dy + k * (NY - 2 * dy)
        dc = r // 2 + k * ((r + 1) % 2 - r // 2)
        return ((y + way * dy + NY) % NY) * NC + (c + dc) % NC

    bar = pltpu.get_barrier_semaphore()
    for dev in [at_zx(dz, d) for dz in (1, -1) for d in range(NX)] + [at_x(d) for d in range(1, NX)]:
        pl.semaphore_signal(bar, inc=1, device_id=dev, device_id_type=MESH)
    for d in range(1, TP):
        pl.semaphore_signal(bar, inc=1, device_id=at_tp((tp + d) % TP), device_id_type=MESH)

    listed_copies = [
        pltpu.make_async_copy(chosen_h, chosen_v, chosen_sem.at[0]),
        pltpu.make_async_copy(chosen_h, chosen_s, chosen_sem.at[1]),
    ]
    for copy in listed_copies:
        copy.start()

    def rows(i):
        return pl.ds(pl.multiple_of(i * CHUNK, CHUNK), CHUNK)

    def tok_copy(i):
        return pltpu.make_async_copy(tok_h.at[rows(i)], x_v.at[rows(i)], tok_sem.at[i])

    w_copies = [
        pltpu.make_async_copy(wk_h, w_v.at[:, 0:128], w_sem.at[0]),
        pltpu.make_async_copy(wv_h, w_v.at[:, 128:256], w_sem.at[1]),
        pltpu.make_async_copy(wq_h, w_v.at[:, 256:512], w_sem.at[2]),
    ]
    w_copies[0].start()
    w_copies[1].start()
    for i in range(NCHUNK):
        tok_copy(i).start()
    wo_copy = pltpu.make_async_copy(wo_h, wfull.at[tp], wo_sem.at[0])
    wo_copy.start()
    w_copies[2].start()

    lane = lax.broadcasted_iota(jnp.int32, (NQB, 128), 1)
    table = jnp.zeros((NQB, 128), jnp.int32)
    for copy in listed_copies:
        copy.wait()
    listed = chosen_v[...]
    for j in range(NFAR):
        col = jnp.broadcast_to(listed[:, j : j + 1], (NQB, 128))
        table = table + jnp.where((col >= 0) & ((col >> 5) == lane), col & (NBLK - 1), 0)
    tab_v[0] = table

    own = {K: own_k, V: own_v}
    up_ref = {(p, j): up_bufs[i] for i, (p, j) in enumerate(UP)}
    dn_ref = {(p, j): dn_bufs[i] for i, (p, j) in enumerate(DOWN)}
    uni = {K: uni_k, V: uni_v}

    def z_copy(own_ref, refs, p, j, half, send, recv, step):
        src, dst, at = own_ref if j == 1 else refs[p, j - 1], refs[p, j], j
        if half is not None:
            blocks = slice(half * (NBLK // 2), (half + 1) * (NBLK // 2))
            src, dst, at = src.at[blocks], dst.at[blocks], 1 - half
        return pltpu.make_async_remote_copy(
            src_ref=src, dst_ref=dst, send_sem=send.at[p, at], recv_sem=recv.at[p, at],
            device_id=at_z(step), device_id_type=MESH,
        )

    def up_copy(p, j, half=None):
        return z_copy(own[p], up_ref, p, j, half, up_send, up_recv, 1)

    def dn_copy(p, j, half=None):
        return z_copy(own[p], dn_ref, p, j, half, dn_send, dn_recv, -1)

    def halves(p, j, first):
        return (0, 1) if (p, j) == (first, 1) else (None,)

    def send_own(half):
        @pl.when(up_arrives(K, 1, z + 1))
        def _():
            up_copy(K, 1, half).start()

        @pl.when(dn_arrives(V, 1, (z + NZ - 1) % NZ))
        def _():
            dn_copy(V, 1, half).start()

        if half == 1:
            send_up(V, 1)
            send_down(K, 1)

    def up_arrives(p, j, here):
        first = LAST if (p, j) == (V, HALF - 1) else j
        return (here >= first) & (here <= LAST)

    def dn_arrives(p, j, here):
        source = (here + j) % NZ
        lands = source <= (HALF - 2 if p == K else HALF - 1)
        if (p, j) in ((K, HALF - 1), (V, HALF)):
            lands = lands & (here != LAST)
        return lands

    def send_up(p, j):
        if (p, j) in up_ref:
            @pl.when(up_arrives(p, j, z + 1))
            def _():
                up_copy(p, j).start()

    def send_down(p, j):
        if (p, j) in dn_ref:
            @pl.when(dn_arrives(p, j, (z + NZ - 1) % NZ))
            def _():
                dn_copy(p, j).start()

    RELAYS = [
        (0, V, HALF - 2, 1, HALF - 2, LAST - 2),
        (1, K, HALF - 1, 1, HALF - 1, LAST - 1),
        (0, K, HALF - 2, -1, 0, 0),
        (1, V, HALF - 1, -1, 0, 0),
    ]

    def relay_x_copy(slot, d, sender_x):
        return pltpu.make_async_remote_copy(
            src_ref=relay_stage.at[slot * (NX - 1) + d - 1], dst_ref=relay_bufs[slot].at[sender_x],
            send_sem=r_send.at[slot, d], recv_sem=r_recv.at[slot, d],
            device_id=at_x(d), device_id_type=MESH,
        )

    def relay_z_copy(slot, p, j, dz, source, second=False):
        send, recv = (up_send, up_recv) if dz == 1 else (dn_send, dn_recv)
        send, recv = (rl_send.at[p], rl_recv.at[p]) if second else (send.at[p, j], recv.at[p, j])
        part = slice(0, NQB) if slot == 0 else slice(FIRST, NQB) if second else slice(0, FIRST)
        return pltpu.make_async_remote_copy(
            src_ref=relay_bufs[slot].at[:, part],
            dst_ref=late_relay[p] if second else uni[p].at[pl.ds(source * NX, NX), part],
            send_sem=send, recv_sem=recv,
            device_id=at_z(dz), device_id_type=MESH,
        )

    def relay_begin(slot, p, buf, source):
        group = source * NX + x

        def pick(i, carry):
            b = block_at(i, 1)
            for d in range(NX):
                block = buf[tab_s[NX + (NX - d) % NX, b, group]]
                if d == 0:
                    relay_bufs[slot][x, i] = block
                else:
                    relay_stage[slot * (NX - 1) + d - 1, i] = block
            return carry

        lax.fori_loop(0, NQB, pick, 0)
        for d in range(1, NX):
            relay_x_copy(slot, d, x).start()

    def relay_end(slot, p, j, dz, source):
        for d in range(1, NX):
            relay_x_copy(slot, d, (x + NX - d) % NX).wait_recv()
        relay_z_copy(slot, p, j + 1, dz, source).start()
        if slot == 1:
            relay_z_copy(slot, p, j + 1, dz, source, True).start()

    def relay_for(p, j, dz):
        for slot, rp, rj, rdz, low, high in RELAYS:
            if (rp, rj, rdz) == (p, j, dz):
                return slot, (z >= low) & (z <= high)
        return None

    def stage_at(a, p, d):
        return (a * 2 + p) * (NX - 1) + d - 1

    def x_copy(a, p, d, source, sender_x, second=False):
        late = LATE.get((a, p))
        part = slice(0, NQB) if late is None else slice(FIRST, NQB) if second else slice(0, FIRST)
        return pltpu.make_async_remote_copy(
            src_ref=stage.at[stage_at(a, p, d), part],
            dst_ref=late_x[late][d - 1] if second else uni[p].at[source * NX + sender_x, part],
            send_sem=xl_send.at[late, d - 1] if second else x_send.at[a, p, d - 1],
            recv_sem=xl_recv.at[late, d - 1] if second else x_recv.at[a, p, d - 1],
            device_id=at_x(d), device_id_type=MESH,
        )

    def spread(a, p, buf, source, mine):
        group = source * NX + x

        def pick(i, carry):
            b = block_at(i, 1)
            for d in range(1, NX):
                stage[stage_at(a, p, d), i] = buf[tab_s[NX - d, b, group]]
            if mine:
                uni[p][group, i] = buf[tab_s[0, b, group]]
            return carry

        lax.fori_loop(0, NQB, pick, 0)
        for d in range(1, NX):
            if mine:
                x_copy(a, p, d, source, x).start()
            else:
                @pl.when(x + d < NX)
                def _():
                    x_copy(a, p, d, source, x).start()

    def each_x(act, second=False):
        for p in (K, V):
            for d in range(1, NX):
                for a, source, when in [(0, z, None)] + [
                    (j, z - j, up_arrives(p, j, z)) for j in range(1, HALF + 1) if (p, j) in up_ref
                ] + [
                    (HALF + j, z + j - NZ, dn_arrives(p, j, z) & (z + j >= NZ)) for j in range(1, HALF + 1) if (p, j) in dn_ref
                ]:
                    if not second or (a, p) in LATE:
                        act(a, p, d, source, when, second)

    w_copies[0].wait()
    w_copies[1].wait()

    def project_kv(i, carry):
        tok_copy(i).wait()
        pair = jnp.dot(x_v[rows(i)], w_v[:, 0:256], preferred_element_type=jnp.float32).astype(jnp.bfloat16)
        blocks = pl.ds(i * (CHUNK // KSPAN), CHUNK // KSPAN)
        own_k[blocks] = pair[:, :HEAD].reshape(CHUNK // KSPAN, KSPAN, HEAD)
        own_v[blocks] = pair[:, HEAD:].reshape(CHUNK // KSPAN, KSPAN, HEAD)

        @pl.when(i == NCHUNK // 2 - 1)
        def _():
            pl.semaphore_wait(bar, 2 * NX + NX - 1 + TP - 1)
            send_own(0)

        return carry

    lax.fori_loop(0, NCHUNK, project_kv, 0)
    send_own(1)

    def tab_copy(d):
        return pltpu.make_async_remote_copy(
            src_ref=tab_v.at[0], dst_ref=tab_v.at[d], send_sem=tab_send.at[d], recv_sem=tab_recv.at[d],
            device_id=at_x(d), device_id_type=MESH,
        )

    def tab_to_smem(d):
        return pltpu.make_async_copy(tab_v.at[d], tab_s.at[d], tab_loc.at[d])

    def tab_relay_copy(d, dz):
        return pltpu.make_async_remote_copy(
            src_ref=tab_v.at[0], dst_ref=tab_v.at[NX + d], send_sem=tab_send.at[NX * (1 if dz < 0 else 2) + d],
            recv_sem=tab_recv.at[NX + d], device_id=at_zx(dz, d), device_id_type=MESH,
        )

    relays = (z == 0) | ((z >= HALF - 2) & (z <= LAST - 1))
    for d in range(1, NX):
        tab_copy(d).start()

    @pl.when(z >= HALF - 1)
    def _():
        for d in range(NX):
            tab_relay_copy(d, -1).start()

    @pl.when(z == LAST)
    def _():
        for d in range(NX):
            tab_relay_copy(d, 1).start()

    tab_to_smem(0).start()

    def wy(slot, sem, dy, lo, hi):
        ref = wfull.at[slot, lo:hi]
        return pltpu.make_async_remote_copy(
            src_ref=ref, dst_ref=ref, send_sem=wy_send.at[sem], recv_sem=wy_recv.at[sem],
            device_id=at_tp(tp_of(dy, 0)), device_id_type=MESH,
        )

    def wd(slot, sem, lo, hi):
        ref = wfull.at[slot, lo:hi]
        return pltpu.make_async_remote_copy(
            src_ref=ref, dst_ref=ref, send_sem=wd_send.at[sem], recv_sem=wd_recv.at[sem],
            device_id=at_tp(tp_of(0, 1)), device_id_type=MESH,
        )

    y_sends = [(tp, 0, 1, 0, QW), (tp, 1, -1, 0, QW), (tp_of(-1, 0), 2, 1, 0, QW // 2), (tp_of(1, 0), 3, -1, QW // 2, QW)]
    y_recvs = [
        (tp_of(-1, 0), 0, 1, 0, QW), (tp_of(1, 0), 1, -1, 0, QW),
        (tp_of(2, 0), 2, 1, 0, QW // 2), (tp_of(2, 0), 3, -1, QW // 2, QW),
    ]
    d_rows = [(0, QW), (0, QW), (0, QW), (0, QW // 2), (QW // 2, QW)]
    d_sends = [(s, i) + d_rows[i] for i, s in enumerate([tp, tp_of(-1, 0), tp_of(1, 0), tp_of(2, 0), tp_of(2, 0)])]
    d_recvs = [(s, i) + d_rows[i] for i, s in enumerate([tp_of(0, 1), tp_of(-1, 1), tp_of(1, 1), tp_of(2, 1), tp_of(2, 1)])]
    wo_copy.wait()
    wy(*y_sends[0]).start()
    wy(*y_sends[1]).start()
    wd(*d_sends[0]).start()


    for d in range(1, NX):
        tab_copy(d).wait_recv()
        tab_to_smem(d).start()
    for d in range(NX):
        tab_to_smem(d).wait()

    @pl.when(relays)
    def _():
        for d in range(NX):
            tab_relay_copy(d, -1).wait_recv()
            tab_to_smem(NX + d).start()
        for d in range(NX):
            tab_to_smem(NX + d).wait()

    spread(0, K, own_k, z, False)
    spread(0, V, own_v, z, False)

    w_copies[2].wait()

    def project_q(i, carry):
        q_v[rows(i)] = jnp.dot(x_v[rows(i)], w_v[:, 256:512], preferred_element_type=jnp.float32).astype(jnp.bfloat16)
        return carry

    lax.fori_loop(0, NCHUNK, project_q, 0)

    def from_below(p, j):
        if (p, j) not in up_ref:
            return

        @pl.when(up_arrives(p, j, z))
        def _():
            for half in halves(p, j, K):
                up_copy(p, j, half).wait_recv()
            send_up(p, j + 1)
            found = relay_for(p, j, 1)
            if found:
                @pl.when(found[1])
                def _():
                    relay_begin(found[0], p, up_ref[p, j], z - j)
            if (p, j) != HELD:
                spread(j, p, up_ref[p, j], z - j, True)
            else:
                @pl.when(jnp.logical_not(found[1]))
                def _():
                    spread(j, p, up_ref[p, j], z - j, True)

    HELD = (V, HALF - 2)

    def spread_held():
        p, j = HELD

        @pl.when(up_arrives(p, j, z) & relay_for(p, j, 1)[1])
        def _():
            spread(j, p, up_ref[p, j], z - j, True)

    def from_above(p, j, rows_now=None):
        if (p, j) not in dn_ref:
            return

        @pl.when(dn_arrives(p, j, z) if rows_now is None else dn_arrives(p, j, z) & rows_now)
        def _():
            for half in halves(p, j, V):
                dn_copy(p, j, half).wait_recv()
            send_down(p, j + 1)
            found = relay_for(p, j, -1)
            if found:
                @pl.when(found[1])
                def _():
                    relay_begin(found[0], p, dn_ref[p, j], z + j)

            @pl.when(z + j >= NZ)
            def _():
                spread(HALF + j, p, dn_ref[p, j], z + j - NZ, True)

    def start_second(a, p, d, source, when, second):
        @pl.when(when)
        def _():
            x_copy(a, p, d, source, x, second).start()

    def end_relays(wanted, rows_now):
        for slot, p, j, dz, low, high in RELAYS:
            if slot == wanted:
                @pl.when((z >= low) & (z <= high) & rows_now)
                def _():
                    relay_end(slot, p, j, dz, z - j if dz == 1 else z + j)

    def weights_far(rows_now):
        @pl.when(rows_now)
        def _():
            for i in (0, 1):
                wy(*y_recvs[i]).wait_recv()
                wy(*y_sends[2 + i]).start()
                wd(*d_sends[1 + i]).start()

    fifth = z == LAST - 2
    for j in range(1, HALF - 2):
        from_above(V, j)
        from_below(K, j)
        from_above(K, j)
        from_below(V, j)
    j = HALF - 2
    from_above(V, j)
    from_below(K, j)
    from_above(K, j)
    from_above(V, j + 1, fifth)
    from_below(V, j)
    weights_far((z <= HALF) | (z == LAST))
    j = HALF - 1
    end_relays(0, z == 0)
    from_above(V, j, jnp.logical_not(fifth))
    from_above(K, j, fifth)
    weights_far((z > HALF) & (z < LAST))
    end_relays(0, z != 0)
    from_below(K, j)
    spread_held()
    from_above(K, j, jnp.logical_not(fifth))
    from_below(V, j)
    j = HALF
    end_relays(1, z == LAST - 1)
    from_above(V, j)
    each_x(start_second, True)
    end_relays(1, z != LAST - 1)
    for i in (2, 3):
        wy(*y_recvs[i]).wait_recv()
        wd(*d_sends[1 + i]).start()

    divided = [
        (0, V, HALF - 1, 1, (z >= HALF - 1) & (z <= LAST - 1)),
        (1, K, HALF, 1, z >= HALF),
        (0, K, HALF - 1, -1, z == LAST),
        (1, V, HALF, -1, z == LAST),
    ]
    def wait_divided(second):
        for slot, p, j, dz, when in divided:
            if slot == 1 or not second:
                @pl.when(when)
                def _():
                    relay_z_copy(slot, p, j, dz, z - j if dz == 1 else z + j - NZ, second).wait_recv()

    def wait_x(a, p, d, source, when, second):
        sender = (x + NX - d) % NX

        @pl.when(sender < x if when is None else when)
        def _():
            x_copy(a, p, d, source, sender, second).wait_recv()

    each_x(wait_x)
    wait_divided(False)

    def place_second(a, p, d, source, when, second):
        @pl.when(when)
        def _():
            uni[p][source * NX + (x + NX - d) % NX, FIRST:NQB] = late_x[LATE[a, p]][d - 1][...]

    far_count = jnp.minimum(kv, NFAR)
    near_row = lax.broadcasted_iota(jnp.int32, (2 * SPAN, SPAN), 0) & (SPAN - 1)
    near_col = lax.broadcasted_iota(jnp.int32, (2 * SPAN, SPAN), 1)
    far_col = lax.broadcasted_iota(jnp.int32, (2 * SPAN, NFAR * KSPAN), 1)

    def att_copy(b, sender):
        return pltpu.make_async_remote_copy(
            src_ref=att.at[b], dst_ref=att_all.at[sender], send_sem=att_send.at[b], recv_sem=att_recv.at[sender],
            device_id=at_tp(b), device_id_type=MESH,
        )

    def attend_block(i, kb, vb):
        b = block_at(i, 1)
        kb[0:SPAN] = own_k[pl.ds(b * (SPAN // KSPAN), SPAN // KSPAN)].reshape(SPAN, HEAD)
        vb[0:SPAN] = own_v[pl.ds(b * (SPAN // KSPAN), SPAN // KSPAN)].reshape(SPAN, HEAD)
        for j in range(NFAR):
            picked = jnp.maximum(chosen_s[b, j], 0)
            kb[SPAN + j * KSPAN : SPAN + (j + 1) * KSPAN] = uni_k[picked >> 5, i]
            block = uni_v[picked >> 5, i]
            vb[SPAN + j * KSPAN : SPAN + (j + 1) * KSPAN] = jnp.where(j < far_count, block, jnp.zeros_like(block))
        q_rows = pl.ds(pl.multiple_of(b * SPAN, SPAN), SPAN)
        qs = jnp.concatenate([q_v[q_rows, 0:HEAD], q_v[q_rows, HEAD:QW]], axis=0)
        scores = lax.dot_general(qs, kb[...], (((1,), (1,)), ((), ())), preferred_element_type=jnp.float32)
        near = jnp.where(near_col <= near_row, scores[:, :SPAN], -jnp.inf)
        far = jnp.where(far_col < far_count * KSPAN, scores[:, SPAN:], -jnp.inf)
        scores = jnp.concatenate([near, far], axis=1) * LOG_SCALE
        top = jnp.max(scores, axis=1, keepdims=True)
        grown = jnp.exp2(scores - top)
        total = jnp.sum(grown, axis=1, keepdims=True)
        weights = (grown * (1.0 / total)).astype(jnp.bfloat16)
        mixed = jnp.dot(weights, vb[...], preferred_element_type=jnp.float32).astype(jnp.bfloat16)
        return jnp.concatenate([mixed[:SPAN], mixed[SPAN:]], axis=1)

    def attend(i, carry):
        @pl.when(i == FIRST // 2)
        def _():
            each_x(wait_x, True)
            wait_divided(True)
            each_x(place_second, True)
            for _, p, j, dz, when in divided[1::2]:
                @pl.when(when)
                def _():
                    source = z - j if dz == 1 else z + j - NZ
                    uni[p][pl.ds(source * NX, NX), FIRST:NQB] = late_relay[p][...]

        first, second = block_at(2 * i, 1), block_at(2 * i + 1, 1)
        one = attend_block(2 * i, kb.at[0], vb.at[0])
        two = attend_block(2 * i + 1, kb.at[1], vb.at[1])
        att[first] = one
        att[second] = two
        att_copy(first, tp).start()

        @pl.when(i < TP // 2 - 1)
        def _():
            att_copy(second, tp).start()

        return carry

    lax.fori_loop(0, TP // 2, attend, 0)

    for args in d_recvs:
        wd(*args).wait_recv()

    def part_of(piece, g):
        return jnp.dot(piece, wfull[g], preferred_element_type=jnp.float32).astype(jnp.bfloat16).astype(jnp.float32)

    def gather(i, carry):
        g, h = block_at(2 * i, -1), block_at(2 * i + 1, -1)
        att_copy(tp, g).wait_recv()
        att_copy(tp, h).wait_recv()
        acc[...] += part_of(att_all[g], g) + part_of(att_all[h], h)
        return carry

    acc[...] = part_of(att[tp], tp)
    lax.fori_loop(0, TP // 2 - 1, gather, 0)
    last = block_at(TP - 2, -1)
    att_copy(tp, last).wait_recv()
    out_ref[...] = (acc[...] + part_of(att_all[last], last)).astype(jnp.bfloat16)

    for d in range(1, NX):
        tab_copy(d).wait_send()

    @pl.when(z >= HALF - 1)
    def _():
        for d in range(NX):
            tab_relay_copy(d, -1).wait_send()

    @pl.when(z == LAST)
    def _():
        for d in range(NX):
            tab_relay_copy(d, 1).wait_send()

    for args in y_sends:
        wy(*args).wait_send()
    for args in d_sends:
        wd(*args).wait_send()
    for (p, j) in up_ref:
        @pl.when(up_arrives(p, j, z + 1))
        def _():
            for half in halves(p, j, K):
                up_copy(p, j, half).wait_send()
    for (p, j) in dn_ref:
        @pl.when(dn_arrives(p, j, (z + NZ - 1) % NZ))
        def _():
            for half in halves(p, j, V):
                dn_copy(p, j, half).wait_send()

    for slot, p, rj, dz, low, high in RELAYS:
        @pl.when((z >= low) & (z <= high))
        def _():
            for d in range(1, NX):
                relay_x_copy(slot, d, x).wait_send()
            relay_z_copy(slot, p, rj + 1, dz, z - rj if dz == 1 else z + rj).wait_send()
            if slot == 1:
                relay_z_copy(slot, p, rj + 1, dz, z - rj if dz == 1 else z + rj, True).wait_send()

    def wait_sent(a, p, d, source, when, second):
        @pl.when(x + d < NX if when is None else when)
        def _():
            x_copy(a, p, d, source, x, second).wait_send()

    each_x(wait_sent)
    each_x(wait_sent, True)

    def att_sent(i, carry):
        b = block_at(i, 1)
        att_copy(b, tp).wait_send()
        return carry

    lax.fori_loop(0, TP - 1, att_sent, 0)


def shards(tokens, query_weight, key_projection_matrix, value_projection_matrix, out_weight, chosen):
    bf16 = jnp.bfloat16
    piece = pltpu.VMEM((NBLK, KSPAN, HEAD), bf16)
    dma = pltpu.SemaphoreType.DMA
    any_space = pl.BlockSpec(memory_space=pl.ANY)
    arrivals = 2 * HALF + 1
    return pl.pallas_call(
        kernel,
        out_shape=pltpu.VMEM((SPAN, WIDTH), bf16),
        in_specs=[any_space] * 6,
        out_specs=pl.BlockSpec(memory_space=pltpu.VMEM),
        scratch_shapes=[
            pltpu.VMEM((NQB, NFAR), jnp.int32),
            pltpu.SMEM((NQB, NFAR), jnp.int32),
            dma((2,)),
            pltpu.VMEM((TOK, WIDTH), bf16),
            pltpu.VMEM((WIDTH, 2 * HEAD + QW), bf16),
            pltpu.VMEM((TP, QW, WIDTH), bf16),
            pltpu.VMEM((TOK, QW), bf16),
            piece,
            piece,
            [piece for _ in UP],
            [piece for _ in DOWN],
            pltpu.VMEM((GROUPS, NQB, KSPAN, HEAD), bf16),
            pltpu.VMEM((GROUPS, NQB, KSPAN, HEAD), bf16),
            pltpu.VMEM((arrivals * 2 * (NX - 1), NQB, KSPAN, HEAD), bf16),
            [pltpu.VMEM((NX, NQB, KSPAN, HEAD), bf16) for _ in range(2)],
            pltpu.VMEM((2 * (NX - 1), NQB, KSPAN, HEAD), bf16),
            [[pltpu.VMEM((FIRST, KSPAN, HEAD), bf16) for _ in range(NX - 1)] for _ in LATE],
            [pltpu.VMEM((NX, FIRST, KSPAN, HEAD), bf16) for _ in range(2)],
            pltpu.VMEM((2 * NX, NQB, 128), jnp.int32),
            pltpu.SMEM((2 * NX, NQB, 128), jnp.int32),
            pltpu.VMEM((2, LISTED, HEAD), bf16),
            pltpu.VMEM((2, LISTED, HEAD), bf16),
            pltpu.VMEM((TP, SPAN, QW), bf16),
            pltpu.VMEM((TP, SPAN, QW), bf16),
            pltpu.VMEM((SPAN, WIDTH), jnp.float32),
            dma((NCHUNK,)), dma((3,)), dma((1,)), dma((3 * NX,)), dma((2 * NX,)), dma((2 * NX,)),
            dma((2, HALF + 1)), dma((2, HALF + 1)), dma((2, HALF + 1)), dma((2, HALF + 1)),
            dma((arrivals, 2, NX - 1)), dma((arrivals, 2, NX - 1)),
            dma((len(LATE), NX - 1)), dma((len(LATE), NX - 1)), dma((2, NX)), dma((2, NX)), dma((2,)), dma((2,)),
            dma((4,)), dma((4,)), dma((5,)), dma((5,)), dma((TP,)), dma((TP,)),
        ],
        compiler_params=pltpu.CompilerParams(
            collective_id=0, has_side_effects=True, vmem_limit_bytes=56 * 2**20
        ),
        name="sparse_attention_layer",
    )(tokens, query_weight, key_projection_matrix, value_projection_matrix, out_weight, chosen)


def solution(mesh):
    return jax.shard_map(
        shards,
        mesh=mesh,
        in_specs=(
            P("kv", None),
            P(None, "tp"),
            P(None, "tp"),
            P(None, "tp"),
            P("tp", None),
            P("kv", None),
        ),
        out_specs=P(("kv", "tp"), None),
        check_vma=False,
    )
```

```python
import functools

import jax
import jax.numpy as jnp
from jax import lax
from jax.experimental import pallas as pl
from jax.experimental.pallas import tpu as pltpu
from jax.sharding import PartitionSpec as P

MESH = pl.DeviceIdType.MESH
NZ, NX, NY, NC = 8, 4, 4, 2
TP = NY * NC
HALF = NZ // 2
HEAD = 128
SPAN = 128
KSPAN = 32
NFAR = 12
TOK = 1024
NBLK = TOK // KSPAN
NQB = TOK // SPAN
WIDTH = 2048
QW = 256
GROUPS = NZ * NX
LISTED = SPAN + NFAR * KSPAN
CHUNK = 512
NCHUNK = TOK // CHUNK
LOG_SCALE = HEAD ** (-0.5) * 1.4426950408889634
K, V = 0, 1
UP = [(p, j) for j in range(1, HALF) for p in (K, V)]
DOWN = [(K, j) for j in range(1, HALF)] + [(V, j) for j in range(1, HALF + 1)]
LAST = NZ - 1
LATE = {(HALF - 1, K): 0, (HALF - 1, V): 1, (2 * HALF - 1, K): 2, (2 * HALF, V): 3}
FIRST = NQB // 2


def kernel(
    tok_h, wq_h, wk_h, wv_h, wo_h, chosen_h,
    out_ref,
    chosen_v, chosen_s, chosen_sem,
    x_v, w_v, wfull, q_v, own_k, own_v, up_bufs, dn_bufs, uni_k, uni_v, stage, relay_bufs, relay_stage, late_x, late_relay,
    tab_v, tab_s, kb, vb, att, att_all, acc,
    tok_sem, w_sem, wo_sem, tab_send, tab_recv, tab_loc,
    up_send, up_recv, dn_send, dn_recv, x_send, x_recv, xl_send, xl_recv, r_send, r_recv, rl_send, rl_recv,
    wy_send, wy_recv, wd_send, wd_recv, att_send, att_recv,
):
    kv = lax.axis_index("kv")
    tp = lax.axis_index("tp")
    z, x = kv // NX, kv % NX
    y, c = tp // NC, tp % NC

    def at_z(step):
        return {"kv": ((z + step + NZ) % NZ) * NX + x, "tp": tp}

    def at_x(step):
        return {"kv": z * NX + (x + step + NX) % NX, "tp": tp}

    def at_zx(dz, dx):
        return {"kv": ((z + dz + NZ) % NZ) * NX + (x + dx) % NX, "tp": tp}

    def at_tp(index):
        return {"kv": kv, "tp": index}

    def tp_of(dy, dc):
        return ((y + dy + NY) % NY) * NC + (c + dc) % NC

    def block_at(i, way):
        r, k = i // 2, i % 2
        dy = 2 - (r + 1) // 2
        dy = dy + k * (NY - 2 * dy)
        dc = r // 2 + k * ((r + 1) % 2 - r // 2)
        return ((y + way * dy + NY) % NY) * NC + (c + dc) % NC

    bar = pltpu.get_barrier_semaphore()
    for dev in [at_zx(dz, d) for dz in (1, -1) for d in range(NX)] + [at_x(d) for d in range(1, NX)]:
        pl.semaphore_signal(bar, inc=1, device_id=dev, device_id_type=MESH)
    for d in range(1, TP):
        pl.semaphore_signal(bar, inc=1, device_id=at_tp((tp + d) % TP), device_id_type=MESH)

    listed_copies = [
        pltpu.make_async_copy(chosen_h, chosen_v, chosen_sem.at[0]),
        pltpu.make_async_copy(chosen_h, chosen_s, chosen_sem.at[1]),
    ]
    for copy in listed_copies:
        copy.start()

    def rows(i):
        return pl.ds(pl.multiple_of(i * CHUNK, CHUNK), CHUNK)

    def tok_copy(i):
        return pltpu.make_async_copy(tok_h.at[rows(i)], x_v.at[rows(i)], tok_sem.at[i])

    w_copies = [
        pltpu.make_async_copy(wk_h, w_v.at[:, 0:128], w_sem.at[0]),
        pltpu.make_async_copy(wv_h, w_v.at[:, 128:256], w_sem.at[1]),
        pltpu.make_async_copy(wq_h, w_v.at[:, 256:512], w_sem.at[2]),
    ]
    w_copies[0].start()
    w_copies[1].start()
    for i in range(NCHUNK):
        tok_copy(i).start()
    wo_copy = pltpu.make_async_copy(wo_h, wfull.at[tp], wo_sem.at[0])
    wo_copy.start()
    w_copies[2].start()

    lane = lax.broadcasted_iota(jnp.int32, (NQB, 128), 1)
    table = jnp.zeros((NQB, 128), jnp.int32)
    for copy in listed_copies:
        copy.wait()
    listed = chosen_v[...]
    for j in range(NFAR):
        col = jnp.broadcast_to(listed[:, j : j + 1], (NQB, 128))
        table = table + jnp.where((col >= 0) & ((col >> 5) == lane), col & (NBLK - 1), 0)
    tab_v[0] = table

    own = {K: own_k, V: own_v}
    up_ref = {(p, j): up_bufs[i] for i, (p, j) in enumerate(UP)}
    dn_ref = {(p, j): dn_bufs[i] for i, (p, j) in enumerate(DOWN)}
    uni = {K: uni_k, V: uni_v}

    def z_copy(own_ref, refs, p, j, half, send, recv, step):
        src, dst, at = own_ref if j == 1 else refs[p, j - 1], refs[p, j], j
        if half is not None:
            blocks = slice(half * (NBLK // 2), (half + 1) * (NBLK // 2))
            src, dst, at = src.at[blocks], dst.at[blocks], 1 - half
        return pltpu.make_async_remote_copy(
            src_ref=src, dst_ref=dst, send_sem=send.at[p, at], recv_sem=recv.at[p, at],
            device_id=at_z(step), device_id_type=MESH,
        )

    def up_copy(p, j, half=None):
        return z_copy(own[p], up_ref, p, j, half, up_send, up_recv, 1)

    def dn_copy(p, j, half=None):
        return z_copy(own[p], dn_ref, p, j, half, dn_send, dn_recv, -1)

    def halves(p, j, first):
        return (0, 1) if (p, j) == (first, 1) else (None,)

    def send_own(half):
        @pl.when(up_arrives(K, 1, z + 1))
        def _():
            up_copy(K, 1, half).start()

        @pl.when(dn_arrives(V, 1, (z + NZ - 1) % NZ))
        def _():
            dn_copy(V, 1, half).start()

        if half == 1:
            send_up(V, 1)
            send_down(K, 1)

    def up_arrives(p, j, here):
        first = LAST if (p, j) == (V, HALF - 1) else j
        return (here >= first) & (here <= LAST)

    def dn_arrives(p, j, here):
        source = (here + j) % NZ
        lands = source <= (HALF - 2 if p == K else HALF - 1)
        if (p, j) in ((K, HALF - 1), (V, HALF)):
            lands = lands & (here != LAST)
        return lands

    def send_up(p, j):
        if (p, j) in up_ref:
            @pl.when(up_arrives(p, j, z + 1))
            def _():
                up_copy(p, j).start()

    def send_down(p, j):
        if (p, j) in dn_ref:
            @pl.when(dn_arrives(p, j, (z + NZ - 1) % NZ))
            def _():
                dn_copy(p, j).start()

    RELAYS = [
        (0, V, HALF - 2, 1, HALF - 2, LAST - 2),
        (1, K, HALF - 1, 1, HALF - 1, LAST - 1),
        (0, K, HALF - 2, -1, 0, 0),
        (1, V, HALF - 1, -1, 0, 0),
    ]

    def relay_x_copy(slot, d, sender_x):
        return pltpu.make_async_remote_copy(
            src_ref=relay_stage.at[slot * (NX - 1) + d - 1], dst_ref=relay_bufs[slot].at[sender_x],
            send_sem=r_send.at[slot, d], recv_sem=r_recv.at[slot, d],
            device_id=at_x(d), device_id_type=MESH,
        )

    def relay_z_copy(slot, p, j, dz, source, second=False):
        send, recv = (up_send, up_recv) if dz == 1 else (dn_send, dn_recv)
        send, recv = (rl_send.at[p], rl_recv.at[p]) if second else (send.at[p, j], recv.at[p, j])
        part = slice(0, NQB) if slot == 0 else slice(FIRST, NQB) if second else slice(0, FIRST)
        return pltpu.make_async_remote_copy(
            src_ref=relay_bufs[slot].at[:, part],
            dst_ref=late_relay[p] if second else uni[p].at[pl.ds(source * NX, NX), part],
            send_sem=send, recv_sem=recv,
            device_id=at_z(dz), device_id_type=MESH,
        )

    def relay_begin(slot, p, buf, source):
        group = source * NX + x

        def pick(i, carry):
            b = block_at(i, 1)
            for d in range(NX):
                block = buf[tab_s[NX + (NX - d) % NX, b, group]]
                if d == 0:
                    relay_bufs[slot][x, i] = block
                else:
                    relay_stage[slot * (NX - 1) + d - 1, i] = block
            return carry

        lax.fori_loop(0, NQB, pick, 0)
        for d in range(1, NX):
            relay_x_copy(slot, d, x).start()

    def relay_end(slot, p, j, dz, source):
        for d in range(1, NX):
            relay_x_copy(slot, d, (x + NX - d) % NX).wait_recv()
        relay_z_copy(slot, p, j + 1, dz, source).start()
        if slot == 1:
            relay_z_copy(slot, p, j + 1, dz, source, True).start()

    def relay_for(p, j, dz):
        for slot, rp, rj, rdz, low, high in RELAYS:
            if (rp, rj, rdz) == (p, j, dz):
                return slot, (z >= low) & (z <= high)
        return None

    def stage_at(a, p, d):
        return (a * 2 + p) * (NX - 1) + d - 1

    def x_copy(a, p, d, source, sender_x, second=False):
        late = LATE.get((a, p))
        part = slice(0, NQB) if late is None else slice(FIRST, NQB) if second else slice(0, FIRST)
        return pltpu.make_async_remote_copy(
            src_ref=stage.at[stage_at(a, p, d), part],
            dst_ref=late_x[late][d - 1] if second else uni[p].at[source * NX + sender_x, part],
            send_sem=xl_send.at[late, d - 1] if second else x_send.at[a, p, d - 1],
            recv_sem=xl_recv.at[late, d - 1] if second else x_recv.at[a, p, d - 1],
            device_id=at_x(d), device_id_type=MESH,
        )

    def spread(a, p, buf, source, mine):
        group = source * NX + x

        def pick(i, carry):
            b = block_at(i, 1)
            for d in range(1, NX):
                stage[stage_at(a, p, d), i] = buf[tab_s[NX - d, b, group]]
            if mine:
                uni[p][group, i] = buf[tab_s[0, b, group]]
            return carry

        lax.fori_loop(0, NQB, pick, 0)
        for d in range(1, NX):
            if mine:
                x_copy(a, p, d, source, x).start()
            else:
                @pl.when(x + d < NX)
                def _():
                    x_copy(a, p, d, source, x).start()

    def each_x(act, second=False):
        for p in (K, V):
            for d in range(1, NX):
                for a, source, when in [(0, z, None)] + [
                    (j, z - j, up_arrives(p, j, z)) for j in range(1, HALF + 1) if (p, j) in up_ref
                ] + [
                    (HALF + j, z + j - NZ, dn_arrives(p, j, z) & (z + j >= NZ)) for j in range(1, HALF + 1) if (p, j) in dn_ref
                ]:
                    if not second or (a, p) in LATE:
                        act(a, p, d, source, when, second)

    w_copies[0].wait()
    w_copies[1].wait()

    def project_kv(i, carry):
        tok_copy(i).wait()
        pair = jnp.dot(x_v[rows(i)], w_v[:, 0:256], preferred_element_type=jnp.float32).astype(jnp.bfloat16)
        blocks = pl.ds(i * (CHUNK // KSPAN), CHUNK // KSPAN)
        own_k[blocks] = pair[:, :HEAD].reshape(CHUNK // KSPAN, KSPAN, HEAD)
        own_v[blocks] = pair[:, HEAD:].reshape(CHUNK // KSPAN, KSPAN, HEAD)

        @pl.when(i == NCHUNK // 2 - 1)
        def _():
            pl.semaphore_wait(bar, 2 * NX + NX - 1 + TP - 1)
            send_own(0)

        return carry

    lax.fori_loop(0, NCHUNK, project_kv, 0)
    send_own(1)

    def tab_copy(d):
        return pltpu.make_async_remote_copy(
            src_ref=tab_v.at[0], dst_ref=tab_v.at[d], send_sem=tab_send.at[d], recv_sem=tab_recv.at[d],
            device_id=at_x(d), device_id_type=MESH,
        )

    def tab_to_smem(d):
        return pltpu.make_async_copy(tab_v.at[d], tab_s.at[d], tab_loc.at[d])

    def tab_relay_copy(d, dz):
        return pltpu.make_async_remote_copy(
            src_ref=tab_v.at[0], dst_ref=tab_v.at[NX + d], send_sem=tab_send.at[NX * (1 if dz < 0 else 2) + d],
            recv_sem=tab_recv.at[NX + d], device_id=at_zx(dz, d), device_id_type=MESH,
        )

    relays = (z == 0) | ((z >= HALF - 2) & (z <= LAST - 1))
    for d in range(1, NX):
        tab_copy(d).start()

    @pl.when(z >= HALF - 1)
    def _():
        for d in range(NX):
            tab_relay_copy(d, -1).start()

    @pl.when(z == LAST)
    def _():
        for d in range(NX):
            tab_relay_copy(d, 1).start()

    tab_to_smem(0).start()

    def wy(slot, sem, dy, lo, hi):
        ref = wfull.at[slot, lo:hi]
        return pltpu.make_async_remote_copy(
            src_ref=ref, dst_ref=ref, send_sem=wy_send.at[sem], recv_sem=wy_recv.at[sem],
            device_id=at_tp(tp_of(dy, 0)), device_id_type=MESH,
        )

    def wd(slot, sem, lo, hi):
        ref = wfull.at[slot, lo:hi]
        return pltpu.make_async_remote_copy(
            src_ref=ref, dst_ref=ref, send_sem=wd_send.at[sem], recv_sem=wd_recv.at[sem],
            device_id=at_tp(tp_of(0, 1)), device_id_type=MESH,
        )

    y_sends = [(tp, 0, 1, 0, QW), (tp, 1, -1, 0, QW), (tp_of(-1, 0), 2, 1, 0, QW // 2), (tp_of(1, 0), 3, -1, QW // 2, QW)]
    y_recvs = [
        (tp_of(-1, 0), 0, 1, 0, QW), (tp_of(1, 0), 1, -1, 0, QW),
        (tp_of(2, 0), 2, 1, 0, QW // 2), (tp_of(2, 0), 3, -1, QW // 2, QW),
    ]
    d_rows = [(0, QW), (0, QW), (0, QW), (0, QW // 2), (QW // 2, QW)]
    d_sends = [(s, i) + d_rows[i] for i, s in enumerate([tp, tp_of(-1, 0), tp_of(1, 0), tp_of(2, 0), tp_of(2, 0)])]
    d_recvs = [(s, i) + d_rows[i] for i, s in enumerate([tp_of(0, 1), tp_of(-1, 1), tp_of(1, 1), tp_of(2, 1), tp_of(2, 1)])]
    wo_copy.wait()
    wy(*y_sends[0]).start()
    wy(*y_sends[1]).start()
    wd(*d_sends[0]).start()


    for d in range(1, NX):
        tab_copy(d).wait_recv()
        tab_to_smem(d).start()
    for d in range(NX):
        tab_to_smem(d).wait()

    @pl.when(relays)
    def _():
        for d in range(NX):
            tab_relay_copy(d, -1).wait_recv()
            tab_to_smem(NX + d).start()
        for d in range(NX):
            tab_to_smem(NX + d).wait()

    spread(0, K, own_k, z, False)
    spread(0, V, own_v, z, False)

    w_copies[2].wait()

    def project_q(i, carry):
        q_v[rows(i)] = jnp.dot(x_v[rows(i)], w_v[:, 256:512], preferred_element_type=jnp.float32).astype(jnp.bfloat16)
        return carry

    lax.fori_loop(0, NCHUNK, project_q, 0)

    def from_below(p, j):
        if (p, j) not in up_ref:
            return

        @pl.when(up_arrives(p, j, z))
        def _():
            for half in halves(p, j, K):
                up_copy(p, j, half).wait_recv()
            send_up(p, j + 1)
            found = relay_for(p, j, 1)
            if found:
                @pl.when(found[1])
                def _():
                    relay_begin(found[0], p, up_ref[p, j], z - j)
            if (p, j) != HELD:
                spread(j, p, up_ref[p, j], z - j, True)
            else:
                @pl.when(jnp.logical_not(found[1]))
                def _():
                    spread(j, p, up_ref[p, j], z - j, True)

    HELD = (V, HALF - 2)

    def spread_held():
        p, j = HELD

        @pl.when(up_arrives(p, j, z) & relay_for(p, j, 1)[1])
        def _():
            spread(j, p, up_ref[p, j], z - j, True)

    def from_above(p, j, rows_now=None):
        if (p, j) not in dn_ref:
            return

        @pl.when(dn_arrives(p, j, z) if rows_now is None else dn_arrives(p, j, z) & rows_now)
        def _():
            for half in halves(p, j, V):
                dn_copy(p, j, half).wait_recv()
            send_down(p, j + 1)
            found = relay_for(p, j, -1)
            if found:
                @pl.when(found[1])
                def _():
                    relay_begin(found[0], p, dn_ref[p, j], z + j)

            @pl.when(z + j >= NZ)
            def _():
                spread(HALF + j, p, dn_ref[p, j], z + j - NZ, True)

    def start_second(a, p, d, source, when, second):
        @pl.when(when)
        def _():
            x_copy(a, p, d, source, x, second).start()

    def end_relays(wanted, rows_now):
        for slot, p, j, dz, low, high in RELAYS:
            if slot == wanted:
                @pl.when((z >= low) & (z <= high) & rows_now)
                def _():
                    relay_end(slot, p, j, dz, z - j if dz == 1 else z + j)

    def weights_far(rows_now):
        @pl.when(rows_now)
        def _():
            for i in (0, 1):
                wy(*y_recvs[i]).wait_recv()
                wy(*y_sends[2 + i]).start()
                wd(*d_sends[1 + i]).start()

    fifth = z == LAST - 2
    for j in range(1, HALF - 2):
        from_above(V, j)
        from_below(K, j)
        from_above(K, j)
        from_below(V, j)
    j = HALF - 2
    from_above(V, j)
    from_below(K, j)
    from_above(K, j)
    from_above(V, j + 1, fifth)
    from_below(V, j)
    weights_far((z <= HALF) | (z == LAST))
    j = HALF - 1
    end_relays(0, z == 0)
    from_above(V, j, jnp.logical_not(fifth))
    from_above(K, j, fifth)
    weights_far((z > HALF) & (z < LAST))
    end_relays(0, z != 0)
    from_below(K, j)
    spread_held()
    from_above(K, j, jnp.logical_not(fifth))
    from_below(V, j)
    j = HALF
    end_relays(1, z == LAST - 1)
    from_above(V, j)
    each_x(start_second, True)
    end_relays(1, z != LAST - 1)
    for i in (2, 3):
        wy(*y_recvs[i]).wait_recv()
        wd(*d_sends[1 + i]).start()

    divided = [
        (0, V, HALF - 1, 1, (z >= HALF - 1) & (z <= LAST - 1)),
        (1, K, HALF, 1, z >= HALF),
        (0, K, HALF - 1, -1, z == LAST),
        (1, V, HALF, -1, z == LAST),
    ]
    def wait_divided(second):
        for slot, p, j, dz, when in divided:
            if slot == 1 or not second:
                @pl.when(when)
                def _():
                    relay_z_copy(slot, p, j, dz, z - j if dz == 1 else z + j - NZ, second).wait_recv()

    def wait_x(a, p, d, source, when, second):
        sender = (x + NX - d) % NX

        @pl.when(sender < x if when is None else when)
        def _():
            x_copy(a, p, d, source, sender, second).wait_recv()

    each_x(wait_x)
    wait_divided(False)

    def place_second(a, p, d, source, when, second):
        @pl.when(when)
        def _():
            uni[p][source * NX + (x + NX - d) % NX, FIRST:NQB] = late_x[LATE[a, p]][d - 1][...]

    far_count = jnp.minimum(kv, NFAR)
    near_row = lax.broadcasted_iota(jnp.int32, (2 * SPAN, SPAN), 0) & (SPAN - 1)
    near_col = lax.broadcasted_iota(jnp.int32, (2 * SPAN, SPAN), 1)
    far_col = lax.broadcasted_iota(jnp.int32, (2 * SPAN, NFAR * KSPAN), 1)

    def att_copy(b, sender):
        return pltpu.make_async_remote_copy(
            src_ref=att.at[b], dst_ref=att_all.at[sender], send_sem=att_send.at[b], recv_sem=att_recv.at[sender],
            device_id=at_tp(b), device_id_type=MESH,
        )

    def attend_block(i, kb, vb):
        b = block_at(i, 1)
        kb[0:SPAN] = own_k[pl.ds(b * (SPAN // KSPAN), SPAN // KSPAN)].reshape(SPAN, HEAD)
        vb[0:SPAN] = own_v[pl.ds(b * (SPAN // KSPAN), SPAN // KSPAN)].reshape(SPAN, HEAD)
        for j in range(NFAR):
            picked = jnp.maximum(chosen_s[b, j], 0)
            kb[SPAN + j * KSPAN : SPAN + (j + 1) * KSPAN] = uni_k[picked >> 5, i]
            block = uni_v[picked >> 5, i]
            vb[SPAN + j * KSPAN : SPAN + (j + 1) * KSPAN] = jnp.where(j < far_count, block, jnp.zeros_like(block))
        q_rows = pl.ds(pl.multiple_of(b * SPAN, SPAN), SPAN)
        qs = jnp.concatenate([q_v[q_rows, 0:HEAD], q_v[q_rows, HEAD:QW]], axis=0)
        scores = lax.dot_general(qs, kb[...], (((1,), (1,)), ((), ())), preferred_element_type=jnp.float32)
        near = jnp.where(near_col <= near_row, scores[:, :SPAN], -jnp.inf)
        far = jnp.where(far_col < far_count * KSPAN, scores[:, SPAN:], -jnp.inf)
        scores = jnp.concatenate([near, far], axis=1) * LOG_SCALE
        top = jnp.max(scores, axis=1, keepdims=True)
        grown = jnp.exp2(scores - top)
        total = jnp.sum(grown, axis=1, keepdims=True)
        weights = (grown * (1.0 / total)).astype(jnp.bfloat16)
        mixed = jnp.dot(weights, vb[...], preferred_element_type=jnp.float32).astype(jnp.bfloat16)
        return jnp.concatenate([mixed[:SPAN], mixed[SPAN:]], axis=1)

    def attend(i, carry):
        @pl.when(i == FIRST // 2)
        def _():
            each_x(wait_x, True)
            wait_divided(True)
            each_x(place_second, True)
            for _, p, j, dz, when in divided[1::2]:
                @pl.when(when)
                def _():
                    source = z - j if dz == 1 else z + j - NZ
                    uni[p][pl.ds(source * NX, NX), FIRST:NQB] = late_relay[p][...]

        first, second = block_at(2 * i, 1), block_at(2 * i + 1, 1)
        one = attend_block(2 * i, kb.at[0], vb.at[0])
        two = attend_block(2 * i + 1, kb.at[1], vb.at[1])
        att[first] = one
        att[second] = two
        att_copy(first, tp).start()

        @pl.when(i < TP // 2 - 1)
        def _():
            att_copy(second, tp).start()

        return carry

    lax.fori_loop(0, TP // 2, attend, 0)

    for args in d_recvs:
        wd(*args).wait_recv()

    def part_of(piece, g):
        return jnp.dot(piece, wfull[g], preferred_element_type=jnp.float32).astype(jnp.bfloat16).astype(jnp.float32)

    def gather(i, carry):
        g, h = block_at(2 * i + 2 * (i // 2), -1), block_at(2 * i + 1 - i // 2, -1)
        att_copy(tp, g).wait_recv()
        att_copy(tp, h).wait_recv()
        acc[...] += part_of(att_all[g], g) + part_of(att_all[h], h)
        return carry

    acc[...] = part_of(att[tp], tp)
    lax.fori_loop(0, TP // 2 - 1, gather, 0)
    last = block_at(TP - 3, -1)
    att_copy(tp, last).wait_recv()
    out_ref[...] = (acc[...] + part_of(att_all[last], last)).astype(jnp.bfloat16)

    for d in range(1, NX):
        tab_copy(d).wait_send()

    @pl.when(z >= HALF - 1)
    def _():
        for d in range(NX):
            tab_relay_copy(d, -1).wait_send()

    @pl.when(z == LAST)
    def _():
        for d in range(NX):
            tab_relay_copy(d, 1).wait_send()

    for args in y_sends:
        wy(*args).wait_send()
    for args in d_sends:
        wd(*args).wait_send()
    for (p, j) in up_ref:
        @pl.when(up_arrives(p, j, z + 1))
        def _():
            for half in halves(p, j, K):
                up_copy(p, j, half).wait_send()
    for (p, j) in dn_ref:
        @pl.when(dn_arrives(p, j, (z + NZ - 1) % NZ))
        def _():
            for half in halves(p, j, V):
                dn_copy(p, j, half).wait_send()

    for slot, p, rj, dz, low, high in RELAYS:
        @pl.when((z >= low) & (z <= high))
        def _():
            for d in range(1, NX):
                relay_x_copy(slot, d, x).wait_send()
            relay_z_copy(slot, p, rj + 1, dz, z - rj if dz == 1 else z + rj).wait_send()
            if slot == 1:
                relay_z_copy(slot, p, rj + 1, dz, z - rj if dz == 1 else z + rj, True).wait_send()

    def wait_sent(a, p, d, source, when, second):
        @pl.when(x + d < NX if when is None else when)
        def _():
            x_copy(a, p, d, source, x, second).wait_send()

    each_x(wait_sent)
    each_x(wait_sent, True)

    def att_sent(i, carry):
        b = block_at(i, 1)
        att_copy(b, tp).wait_send()
        return carry

    lax.fori_loop(0, TP - 1, att_sent, 0)


def shards(tokens, query_weight, key_projection_matrix, value_projection_matrix, out_weight, chosen):
    bf16 = jnp.bfloat16
    piece = pltpu.VMEM((NBLK, KSPAN, HEAD), bf16)
    dma = pltpu.SemaphoreType.DMA
    any_space = pl.BlockSpec(memory_space=pl.ANY)
    arrivals = 2 * HALF + 1
    return pl.pallas_call(
        kernel,
        out_shape=pltpu.VMEM((SPAN, WIDTH), bf16),
        in_specs=[any_space] * 6,
        out_specs=pl.BlockSpec(memory_space=pltpu.VMEM),
        scratch_shapes=[
            pltpu.VMEM((NQB, NFAR), jnp.int32),
            pltpu.SMEM((NQB, NFAR), jnp.int32),
            dma((2,)),
            pltpu.VMEM((TOK, WIDTH), bf16),
            pltpu.VMEM((WIDTH, 2 * HEAD + QW), bf16),
            pltpu.VMEM((TP, QW, WIDTH), bf16),
            pltpu.VMEM((TOK, QW), bf16),
            piece,
            piece,
            [piece for _ in UP],
            [piece for _ in DOWN],
            pltpu.VMEM((GROUPS, NQB, KSPAN, HEAD), bf16),
            pltpu.VMEM((GROUPS, NQB, KSPAN, HEAD), bf16),
            pltpu.VMEM((arrivals * 2 * (NX - 1), NQB, KSPAN, HEAD), bf16),
            [pltpu.VMEM((NX, NQB, KSPAN, HEAD), bf16) for _ in range(2)],
            pltpu.VMEM((2 * (NX - 1), NQB, KSPAN, HEAD), bf16),
            [[pltpu.VMEM((FIRST, KSPAN, HEAD), bf16) for _ in range(NX - 1)] for _ in LATE],
            [pltpu.VMEM((NX, FIRST, KSPAN, HEAD), bf16) for _ in range(2)],
            pltpu.VMEM((2 * NX, NQB, 128), jnp.int32),
            pltpu.SMEM((2 * NX, NQB, 128), jnp.int32),
            pltpu.VMEM((2, LISTED, HEAD), bf16),
            pltpu.VMEM((2, LISTED, HEAD), bf16),
            pltpu.VMEM((TP, SPAN, QW), bf16),
            pltpu.VMEM((TP, SPAN, QW), bf16),
            pltpu.VMEM((SPAN, WIDTH), jnp.float32),
            dma((NCHUNK,)), dma((3,)), dma((1,)), dma((3 * NX,)), dma((2 * NX,)), dma((2 * NX,)),
            dma((2, HALF + 1)), dma((2, HALF + 1)), dma((2, HALF + 1)), dma((2, HALF + 1)),
            dma((arrivals, 2, NX - 1)), dma((arrivals, 2, NX - 1)),
            dma((len(LATE), NX - 1)), dma((len(LATE), NX - 1)), dma((2, NX)), dma((2, NX)), dma((2,)), dma((2,)),
            dma((4,)), dma((4,)), dma((5,)), dma((5,)), dma((TP,)), dma((TP,)),
        ],
        compiler_params=pltpu.CompilerParams(
            collective_id=0, has_side_effects=True, vmem_limit_bytes=56 * 2**20
        ),
        name="sparse_attention_layer",
    )(tokens, query_weight, key_projection_matrix, value_projection_matrix, out_weight, chosen)


def solution(mesh):
    return jax.shard_map(
        shards,
        mesh=mesh,
        in_specs=(
            P("kv", None),
            P(None, "tp"),
            P(None, "tp"),
            P(None, "tp"),
            P("tp", None),
            P("kv", None),
        ),
        out_specs=P(("kv", "tp"), None),
        check_vma=False,
    )
```

```python
import functools

import jax
import jax.numpy as jnp
from jax import lax
from jax.experimental import pallas as pl
from jax.experimental.pallas import tpu as pltpu
from jax.sharding import PartitionSpec as P

MESH = pl.DeviceIdType.MESH
NZ, NX, NY, NC = 8, 4, 4, 2
TP = NY * NC
HALF = NZ // 2
HEAD = 128
SPAN = 128
KSPAN = 32
NFAR = 12
TOK = 1024
NBLK = TOK // KSPAN
NQB = TOK // SPAN
WIDTH = 2048
QW = 256
GROUPS = NZ * NX
LISTED = SPAN + NFAR * KSPAN
CHUNK = 512
NCHUNK = TOK // CHUNK
LOG_SCALE = HEAD ** (-0.5) * 1.4426950408889634
K, V = 0, 1
UP = [(p, j) for j in range(1, HALF) for p in (K, V)]
DOWN = [(K, j) for j in range(1, HALF)] + [(V, j) for j in range(1, HALF + 1)]
LAST = NZ - 1
LATE = {(HALF - 1, K): 0, (HALF - 1, V): 1, (2 * HALF - 1, K): 2, (2 * HALF, V): 3}
FIRST = NQB // 2


def kernel(
    tok_h, wq_h, wk_h, wv_h, wo_h, chosen_h,
    out_ref,
    chosen_v, chosen_s, chosen_sem,
    x_v, w_v, wfull, q_v, own_k, own_v, up_bufs, dn_bufs, uni_k, uni_v, stage, relay_bufs, relay_stage, late_x, late_relay,
    tab_v, tab_s, kb, vb, att, att_all, acc,
    tok_sem, w_sem, wo_sem, tab_send, tab_recv, tab_loc,
    up_send, up_recv, dn_send, dn_recv, x_send, x_recv, xl_send, xl_recv, r_send, r_recv, rl_send, rl_recv,
    wy_send, wy_recv, wd_send, wd_recv, att_send, att_recv,
):
    kv = lax.axis_index("kv")
    tp = lax.axis_index("tp")
    z, x = kv // NX, kv % NX
    y, c = tp // NC, tp % NC

    def at_z(step):
        return {"kv": ((z + step + NZ) % NZ) * NX + x, "tp": tp}

    def at_x(step):
        return {"kv": z * NX + (x + step + NX) % NX, "tp": tp}

    def at_zx(dz, dx):
        return {"kv": ((z + dz + NZ) % NZ) * NX + (x + dx) % NX, "tp": tp}

    def at_tp(index):
        return {"kv": kv, "tp": index}

    def tp_of(dy, dc):
        return ((y + dy + NY) % NY) * NC + (c + dc) % NC

    def block_at(i, way):
        r, k = i // 2, i % 2
        dy = 2 - (r + 1) // 2
        dy = dy + k * (NY - 2 * dy)
        dc = r // 2 + k * ((r + 1) % 2 - r // 2)
        return ((y + way * dy + NY) % NY) * NC + (c + dc) % NC

    bar = pltpu.get_barrier_semaphore()
    for dev in [at_zx(dz, d) for dz in (1, -1) for d in range(NX)] + [at_x(d) for d in range(1, NX)]:
        pl.semaphore_signal(bar, inc=1, device_id=dev, device_id_type=MESH)
    for d in range(1, TP):
        pl.semaphore_signal(bar, inc=1, device_id=at_tp((tp + d) % TP), device_id_type=MESH)

    listed_copies = [
        pltpu.make_async_copy(chosen_h, chosen_v, chosen_sem.at[0]),
        pltpu.make_async_copy(chosen_h, chosen_s, chosen_sem.at[1]),
    ]
    for copy in listed_copies:
        copy.start()

    def rows(i):
        return pl.ds(pl.multiple_of(i * CHUNK, CHUNK), CHUNK)

    def tok_copy(i):
        return pltpu.make_async_copy(tok_h.at[rows(i)], x_v.at[rows(i)], tok_sem.at[i])

    w_copies = [
        pltpu.make_async_copy(wk_h, w_v.at[:, 0:128], w_sem.at[0]),
        pltpu.make_async_copy(wv_h, w_v.at[:, 128:256], w_sem.at[1]),
        pltpu.make_async_copy(wq_h, w_v.at[:, 256:512], w_sem.at[2]),
    ]
    w_copies[0].start()
    w_copies[1].start()
    for i in range(NCHUNK):
        tok_copy(i).start()
    wo_copy = pltpu.make_async_copy(wo_h, wfull.at[tp], wo_sem.at[0])
    wo_copy.start()
    w_copies[2].start()

    lane = lax.broadcasted_iota(jnp.int32, (NQB, 128), 1)
    table = jnp.zeros((NQB, 128), jnp.int32)
    for copy in listed_copies:
        copy.wait()
    listed = chosen_v[...]
    for j in range(NFAR):
        col = jnp.broadcast_to(listed[:, j : j + 1], (NQB, 128))
        table = table + jnp.where((col >= 0) & ((col >> 5) == lane), col & (NBLK - 1), 0)
    tab_v[0] = table

    own = {K: own_k, V: own_v}
    up_ref = {(p, j): up_bufs[i] for i, (p, j) in enumerate(UP)}
    dn_ref = {(p, j): dn_bufs[i] for i, (p, j) in enumerate(DOWN)}
    uni = {K: uni_k, V: uni_v}

    def z_copy(own_ref, refs, p, j, half, send, recv, step):
        src, dst, at = own_ref if j == 1 else refs[p, j - 1], refs[p, j], j
        if half is not None:
            blocks = slice(half * (NBLK // 2), (half + 1) * (NBLK // 2))
            src, dst, at = src.at[blocks], dst.at[blocks], 1 - half
        return pltpu.make_async_remote_copy(
            src_ref=src, dst_ref=dst, send_sem=send.at[p, at], recv_sem=recv.at[p, at],
            device_id=at_z(step), device_id_type=MESH,
        )

    def up_copy(p, j, half=None):
        return z_copy(own[p], up_ref, p, j, half, up_send, up_recv, 1)

    def dn_copy(p, j, half=None):
        return z_copy(own[p], dn_ref, p, j, half, dn_send, dn_recv, -1)

    def halves(p, j, first):
        return (0, 1) if (p, j) == (first, 1) else (None,)

    def send_own(half):
        @pl.when(up_arrives(K, 1, z + 1))
        def _():
            up_copy(K, 1, half).start()

        @pl.when(dn_arrives(V, 1, (z + NZ - 1) % NZ))
        def _():
            dn_copy(V, 1, half).start()

        if half == 1:
            send_up(V, 1)
            send_down(K, 1)

    def up_arrives(p, j, here):
        first = LAST if (p, j) == (V, HALF - 1) else j
        return (here >= first) & (here <= LAST)

    def dn_arrives(p, j, here):
        source = (here + j) % NZ
        lands = source <= (HALF - 2 if p == K else HALF - 1)
        if (p, j) in ((K, HALF - 1), (V, HALF)):
            lands = lands & (here != LAST)
        return lands

    def send_up(p, j):
        if (p, j) in up_ref:
            @pl.when(up_arrives(p, j, z + 1))
            def _():
                up_copy(p, j).start()

    def send_down(p, j):
        if (p, j) in dn_ref:
            @pl.when(dn_arrives(p, j, (z + NZ - 1) % NZ))
            def _():
                dn_copy(p, j).start()

    RELAYS = [
        (0, V, HALF - 2, 1, HALF - 2, LAST - 2),
        (1, K, HALF - 1, 1, HALF - 1, LAST - 1),
        (0, K, HALF - 2, -1, 0, 0),
        (1, V, HALF - 1, -1, 0, 0),
    ]

    def relay_x_copy(slot, d, sender_x):
        return pltpu.make_async_remote_copy(
            src_ref=relay_stage.at[slot * (NX - 1) + d - 1], dst_ref=relay_bufs[slot].at[sender_x],
            send_sem=r_send.at[slot, d], recv_sem=r_recv.at[slot, d],
            device_id=at_x(d), device_id_type=MESH,
        )

    def relay_z_copy(slot, p, j, dz, source, second=False):
        send, recv = (up_send, up_recv) if dz == 1 else (dn_send, dn_recv)
        send, recv = (rl_send.at[p], rl_recv.at[p]) if second else (send.at[p, j], recv.at[p, j])
        part = slice(0, NQB) if slot == 0 else slice(FIRST, NQB) if second else slice(0, FIRST)
        return pltpu.make_async_remote_copy(
            src_ref=relay_bufs[slot].at[:, part],
            dst_ref=late_relay[p] if second else uni[p].at[pl.ds(source * NX, NX), part],
            send_sem=send, recv_sem=recv,
            device_id=at_z(dz), device_id_type=MESH,
        )

    def relay_begin(slot, p, buf, source):
        group = source * NX + x

        def pick(i, carry):
            b = block_at(i, 1)
            for d in range(NX):
                block = buf[tab_s[NX + (NX - d) % NX, b, group]]
                if d == 0:
                    relay_bufs[slot][x, i] = block
                else:
                    relay_stage[slot * (NX - 1) + d - 1, i] = block
            return carry

        lax.fori_loop(0, NQB, pick, 0)
        for d in range(1, NX):
            relay_x_copy(slot, d, x).start()

    def relay_end(slot, p, j, dz, source):
        for d in range(1, NX):
            relay_x_copy(slot, d, (x + NX - d) % NX).wait_recv()
        relay_z_copy(slot, p, j + 1, dz, source).start()
        if slot == 1:
            relay_z_copy(slot, p, j + 1, dz, source, True).start()

    def relay_for(p, j, dz):
        for slot, rp, rj, rdz, low, high in RELAYS:
            if (rp, rj, rdz) == (p, j, dz):
                return slot, (z >= low) & (z <= high)
        return None

    def stage_at(a, p, d):
        return (a * 2 + p) * (NX - 1) + d - 1

    def x_copy(a, p, d, source, sender_x, second=False):
        late = LATE.get((a, p))
        part = slice(0, NQB) if late is None else slice(FIRST, NQB) if second else slice(0, FIRST)
        return pltpu.make_async_remote_copy(
            src_ref=stage.at[stage_at(a, p, d), part],
            dst_ref=late_x[late][d - 1] if second else uni[p].at[source * NX + sender_x, part],
            send_sem=xl_send.at[late, d - 1] if second else x_send.at[a, p, d - 1],
            recv_sem=xl_recv.at[late, d - 1] if second else x_recv.at[a, p, d - 1],
            device_id=at_x(d), device_id_type=MESH,
        )

    def spread(a, p, buf, source, mine):
        group = source * NX + x

        def pick(i, carry):
            b = block_at(i, 1)
            for d in range(1, NX):
                stage[stage_at(a, p, d), i] = buf[tab_s[NX - d, b, group]]
            if mine:
                uni[p][group, i] = buf[tab_s[0, b, group]]
            return carry

        lax.fori_loop(0, NQB, pick, 0)
        for d in range(1, NX):
            if mine:
                x_copy(a, p, d, source, x).start()
            else:
                @pl.when(x + d < NX)
                def _():
                    x_copy(a, p, d, source, x).start()

    def each_x(act, second=False):
        for p in (K, V):
            for d in range(1, NX):
                for a, source, when in [(0, z, None)] + [
                    (j, z - j, up_arrives(p, j, z)) for j in range(1, HALF + 1) if (p, j) in up_ref
                ] + [
                    (HALF + j, z + j - NZ, dn_arrives(p, j, z) & (z + j >= NZ)) for j in range(1, HALF + 1) if (p, j) in dn_ref
                ]:
                    if not second or (a, p) in LATE:
                        act(a, p, d, source, when, second)

    w_copies[0].wait()
    w_copies[1].wait()

    def project_kv(i, carry):
        tok_copy(i).wait()
        pair = jnp.dot(x_v[rows(i)], w_v[:, 0:256], preferred_element_type=jnp.float32).astype(jnp.bfloat16)
        blocks = pl.ds(i * (CHUNK // KSPAN), CHUNK // KSPAN)
        own_k[blocks] = pair[:, :HEAD].reshape(CHUNK // KSPAN, KSPAN, HEAD)
        own_v[blocks] = pair[:, HEAD:].reshape(CHUNK // KSPAN, KSPAN, HEAD)

        @pl.when(i == NCHUNK // 2 - 1)
        def _():
            pl.semaphore_wait(bar, 2 * NX + NX - 1 + TP - 1)
            send_own(0)

        return carry

    lax.fori_loop(0, NCHUNK, project_kv, 0)
    send_own(1)

    def tab_copy(d):
        return pltpu.make_async_remote_copy(
            src_ref=tab_v.at[0], dst_ref=tab_v.at[d], send_sem=tab_send.at[d], recv_sem=tab_recv.at[d],
            device_id=at_x(d), device_id_type=MESH,
        )

    def tab_to_smem(d):
        return pltpu.make_async_copy(tab_v.at[d], tab_s.at[d], tab_loc.at[d])

    def tab_relay_copy(d, dz):
        return pltpu.make_async_remote_copy(
            src_ref=tab_v.at[0], dst_ref=tab_v.at[NX + d], send_sem=tab_send.at[NX * (1 if dz < 0 else 2) + d],
            recv_sem=tab_recv.at[NX + d], device_id=at_zx(dz, d), device_id_type=MESH,
        )

    relays = (z == 0) | ((z >= HALF - 2) & (z <= LAST - 1))
    for d in range(1, NX):
        tab_copy(d).start()

    @pl.when(z >= HALF - 1)
    def _():
        for d in range(NX):
            tab_relay_copy(d, -1).start()

    @pl.when(z == LAST)
    def _():
        for d in range(NX):
            tab_relay_copy(d, 1).start()

    tab_to_smem(0).start()

    def wy(slot, sem, dy, lo, hi):
        ref = wfull.at[slot, lo:hi]
        return pltpu.make_async_remote_copy(
            src_ref=ref, dst_ref=ref, send_sem=wy_send.at[sem], recv_sem=wy_recv.at[sem],
            device_id=at_tp(tp_of(dy, 0)), device_id_type=MESH,
        )

    def wd(slot, sem, lo, hi):
        ref = wfull.at[slot, lo:hi]
        return pltpu.make_async_remote_copy(
            src_ref=ref, dst_ref=ref, send_sem=wd_send.at[sem], recv_sem=wd_recv.at[sem],
            device_id=at_tp(tp_of(0, 1)), device_id_type=MESH,
        )

    y_sends = [(tp, 0, 1, 0, QW), (tp, 1, -1, 0, QW), (tp_of(-1, 0), 2, 1, 0, QW // 2), (tp_of(1, 0), 3, -1, QW // 2, QW)]
    y_recvs = [
        (tp_of(-1, 0), 0, 1, 0, QW), (tp_of(1, 0), 1, -1, 0, QW),
        (tp_of(2, 0), 2, 1, 0, QW // 2), (tp_of(2, 0), 3, -1, QW // 2, QW),
    ]
    d_rows = [(0, QW), (0, QW), (0, QW), (0, QW // 2), (QW // 2, QW)]
    d_sends = [(s, i) + d_rows[i] for i, s in enumerate([tp, tp_of(-1, 0), tp_of(1, 0), tp_of(2, 0), tp_of(2, 0)])]
    d_recvs = [(s, i) + d_rows[i] for i, s in enumerate([tp_of(0, 1), tp_of(-1, 1), tp_of(1, 1), tp_of(2, 1), tp_of(2, 1)])]
    wo_copy.wait()
    wy(*y_sends[0]).start()
    wy(*y_sends[1]).start()
    wd(*d_sends[0]).start()


    for d in range(1, NX):
        tab_copy(d).wait_recv()
        tab_to_smem(d).start()
    for d in range(NX):
        tab_to_smem(d).wait()

    @pl.when(relays)
    def _():
        for d in range(NX):
            tab_relay_copy(d, -1).wait_recv()
            tab_to_smem(NX + d).start()
        for d in range(NX):
            tab_to_smem(NX + d).wait()

    spread(0, K, own_k, z, False)
    spread(0, V, own_v, z, False)

    w_copies[2].wait()

    def project_q(i, carry):
        q_v[rows(i)] = jnp.dot(x_v[rows(i)], w_v[:, 256:512], preferred_element_type=jnp.float32).astype(jnp.bfloat16)
        return carry

    lax.fori_loop(0, NCHUNK, project_q, 0)

    def from_below(p, j):
        if (p, j) not in up_ref:
            return

        @pl.when(up_arrives(p, j, z))
        def _():
            for half in halves(p, j, K):
                up_copy(p, j, half).wait_recv()
            send_up(p, j + 1)
            found = relay_for(p, j, 1)
            if found:
                @pl.when(found[1])
                def _():
                    relay_begin(found[0], p, up_ref[p, j], z - j)
            if (p, j) != HELD:
                spread(j, p, up_ref[p, j], z - j, True)
            else:
                @pl.when(jnp.logical_not(found[1]))
                def _():
                    spread(j, p, up_ref[p, j], z - j, True)

    HELD = (V, HALF - 2)

    def spread_held():
        p, j = HELD

        @pl.when(up_arrives(p, j, z) & relay_for(p, j, 1)[1])
        def _():
            spread(j, p, up_ref[p, j], z - j, True)

    def from_above(p, j, rows_now=None):
        if (p, j) not in dn_ref:
            return

        @pl.when(dn_arrives(p, j, z) if rows_now is None else dn_arrives(p, j, z) & rows_now)
        def _():
            for half in halves(p, j, V):
                dn_copy(p, j, half).wait_recv()
            send_down(p, j + 1)
            found = relay_for(p, j, -1)
            if found:
                @pl.when(found[1])
                def _():
                    relay_begin(found[0], p, dn_ref[p, j], z + j)

            @pl.when(z + j >= NZ)
            def _():
                spread(HALF + j, p, dn_ref[p, j], z + j - NZ, True)

    def start_second(a, p, d, source, when, second):
        @pl.when(when)
        def _():
            x_copy(a, p, d, source, x, second).start()

    def end_relays(wanted, rows_now):
        for slot, p, j, dz, low, high in RELAYS:
            if slot == wanted:
                @pl.when((z >= low) & (z <= high) & rows_now)
                def _():
                    relay_end(slot, p, j, dz, z - j if dz == 1 else z + j)

    def weights_far(rows_now):
        @pl.when(rows_now)
        def _():
            for i in (0, 1):
                wy(*y_recvs[i]).wait_recv()
                wy(*y_sends[2 + i]).start()
                wd(*d_sends[1 + i]).start()

    fifth = z == LAST - 2
    for j in range(1, HALF - 2):
        from_above(V, j)
        from_below(K, j)
        from_above(K, j)
        from_below(V, j)
    j = HALF - 2
    from_above(V, j)
    from_below(K, j)
    from_above(K, j)
    from_above(V, j + 1, fifth)
    from_below(V, j)
    weights_far((z <= HALF) | (z == LAST))
    j = HALF - 1
    end_relays(0, z == 0)
    from_above(V, j, jnp.logical_not(fifth))
    from_above(K, j, fifth)
    weights_far((z > HALF) & (z < LAST))
    end_relays(0, z != 0)
    from_below(K, j)
    spread_held()
    from_above(K, j, jnp.logical_not(fifth))
    from_below(V, j)
    j = HALF
    end_relays(1, z == LAST - 1)
    from_above(V, j)
    each_x(start_second, True)
    end_relays(1, z != LAST - 1)
    for i in (2, 3):
        wy(*y_recvs[i]).wait_recv()
        wd(*d_sends[1 + i]).start()

    divided = [
        (0, V, HALF - 1, 1, (z >= HALF - 1) & (z <= LAST - 1)),
        (1, K, HALF, 1, z >= HALF),
        (0, K, HALF - 1, -1, z == LAST),
        (1, V, HALF, -1, z == LAST),
    ]
    def wait_divided(second):
        for slot, p, j, dz, when in divided:
            if slot == 1 or not second:
                @pl.when(when)
                def _():
                    relay_z_copy(slot, p, j, dz, z - j if dz == 1 else z + j - NZ, second).wait_recv()

    def wait_x(a, p, d, source, when, second):
        sender = (x + NX - d) % NX

        @pl.when(sender < x if when is None else when)
        def _():
            x_copy(a, p, d, source, sender, second).wait_recv()

    each_x(wait_x)
    wait_divided(False)

    def place_second(a, p, d, source, when, second):
        @pl.when(when)
        def _():
            uni[p][source * NX + (x + NX - d) % NX, FIRST:NQB] = late_x[LATE[a, p]][d - 1][...]

    far_count = jnp.minimum(kv, NFAR)
    near_row = lax.broadcasted_iota(jnp.int32, (2 * SPAN, SPAN), 0) & (SPAN - 1)
    near_col = lax.broadcasted_iota(jnp.int32, (2 * SPAN, SPAN), 1)
    far_col = lax.broadcasted_iota(jnp.int32, (2 * SPAN, NFAR * KSPAN), 1)

    def att_copy(b, sender):
        return pltpu.make_async_remote_copy(
            src_ref=att.at[b], dst_ref=att_all.at[sender], send_sem=att_send.at[b], recv_sem=att_recv.at[sender],
            device_id=at_tp(b), device_id_type=MESH,
        )

    def attend_block(i, kb, vb):
        b = block_at(i, 1)
        kb[0:SPAN] = own_k[pl.ds(b * (SPAN // KSPAN), SPAN // KSPAN)].reshape(SPAN, HEAD)
        vb[0:SPAN] = own_v[pl.ds(b * (SPAN // KSPAN), SPAN // KSPAN)].reshape(SPAN, HEAD)
        for j in range(NFAR):
            picked = jnp.maximum(chosen_s[b, j], 0)
            kb[SPAN + j * KSPAN : SPAN + (j + 1) * KSPAN] = uni_k[picked >> 5, i]
            block = uni_v[picked >> 5, i]
            vb[SPAN + j * KSPAN : SPAN + (j + 1) * KSPAN] = jnp.where(j < far_count, block, jnp.zeros_like(block))
        q_rows = pl.ds(pl.multiple_of(b * SPAN, SPAN), SPAN)
        qs = jnp.concatenate([q_v[q_rows, 0:HEAD], q_v[q_rows, HEAD:QW]], axis=0)
        scores = lax.dot_general(qs, kb[...], (((1,), (1,)), ((), ())), preferred_element_type=jnp.float32)
        near = jnp.where(near_col <= near_row, scores[:, :SPAN], -jnp.inf)
        far = jnp.where(far_col < far_count * KSPAN, scores[:, SPAN:], -jnp.inf)
        scores = jnp.concatenate([near, far], axis=1) * LOG_SCALE
        top = jnp.max(scores, axis=1, keepdims=True)
        grown = jnp.exp2(scores - top)
        total = jnp.sum(grown, axis=1, keepdims=True)
        weights = (grown * (1.0 / total)).astype(jnp.bfloat16)
        mixed = jnp.dot(weights, vb[...], preferred_element_type=jnp.float32).astype(jnp.bfloat16)
        return jnp.concatenate([mixed[:SPAN], mixed[SPAN:]], axis=1)

    def attend(i, carry):
        @pl.when(i == FIRST // 2)
        def _():
            each_x(wait_x, True)
            wait_divided(True)
            each_x(place_second, True)
            for _, p, j, dz, when in divided[1::2]:
                @pl.when(when)
                def _():
                    source = z - j if dz == 1 else z + j - NZ
                    uni[p][pl.ds(source * NX, NX), FIRST:NQB] = late_relay[p][...]

        first, second = block_at(2 * i, 1), block_at(2 * i + 1, 1)
        att[first] = attend_block(2 * i, kb.at[0], vb.at[0])
        att_copy(first, tp).start()
        att[second] = attend_block(2 * i + 1, kb.at[1], vb.at[1])

        @pl.when(i < TP // 2 - 1)
        def _():
            att_copy(second, tp).start()

        return carry

    lax.fori_loop(0, TP // 2, attend, 0)

    for args in d_recvs:
        wd(*args).wait_recv()

    def part_of(piece, g):
        return jnp.dot(piece, wfull[g], preferred_element_type=jnp.float32).astype(jnp.bfloat16).astype(jnp.float32)

    def gather(i, carry):
        g, h = block_at(2 * i + 2 * (i // 2), -1), block_at(2 * i + 1 - i // 2, -1)
        att_copy(tp, g).wait_recv()
        att_copy(tp, h).wait_recv()
        acc[...] += part_of(att_all[g], g) + part_of(att_all[h], h)
        return carry

    acc[...] = part_of(att[tp], tp)
    lax.fori_loop(0, TP // 2 - 1, gather, 0)
    last = block_at(TP - 3, -1)
    att_copy(tp, last).wait_recv()
    out_ref[...] = (acc[...] + part_of(att_all[last], last)).astype(jnp.bfloat16)

    for d in range(1, NX):
        tab_copy(d).wait_send()

    @pl.when(z >= HALF - 1)
    def _():
        for d in range(NX):
            tab_relay_copy(d, -1).wait_send()

    @pl.when(z == LAST)
    def _():
        for d in range(NX):
            tab_relay_copy(d, 1).wait_send()

    for args in y_sends:
        wy(*args).wait_send()
    for args in d_sends:
        wd(*args).wait_send()
    for (p, j) in up_ref:
        @pl.when(up_arrives(p, j, z + 1))
        def _():
            for half in halves(p, j, K):
                up_copy(p, j, half).wait_send()
    for (p, j) in dn_ref:
        @pl.when(dn_arrives(p, j, (z + NZ - 1) % NZ))
        def _():
            for half in halves(p, j, V):
                dn_copy(p, j, half).wait_send()

    for slot, p, rj, dz, low, high in RELAYS:
        @pl.when((z >= low) & (z <= high))
        def _():
            for d in range(1, NX):
                relay_x_copy(slot, d, x).wait_send()
            relay_z_copy(slot, p, rj + 1, dz, z - rj if dz == 1 else z + rj).wait_send()
            if slot == 1:
                relay_z_copy(slot, p, rj + 1, dz, z - rj if dz == 1 else z + rj, True).wait_send()

    def wait_sent(a, p, d, source, when, second):
        @pl.when(x + d < NX if when is None else when)
        def _():
            x_copy(a, p, d, source, x, second).wait_send()

    each_x(wait_sent)
    each_x(wait_sent, True)

    def att_sent(i, carry):
        b = block_at(i, 1)
        att_copy(b, tp).wait_send()
        return carry

    lax.fori_loop(0, TP - 1, att_sent, 0)


def shards(tokens, query_weight, key_projection_matrix, value_projection_matrix, out_weight, chosen):
    bf16 = jnp.bfloat16
    piece = pltpu.VMEM((NBLK, KSPAN, HEAD), bf16)
    dma = pltpu.SemaphoreType.DMA
    any_space = pl.BlockSpec(memory_space=pl.ANY)
    arrivals = 2 * HALF + 1
    return pl.pallas_call(
        kernel,
        out_shape=pltpu.VMEM((SPAN, WIDTH), bf16),
        in_specs=[any_space] * 6,
        out_specs=pl.BlockSpec(memory_space=pltpu.VMEM),
        scratch_shapes=[
            pltpu.VMEM((NQB, NFAR), jnp.int32),
            pltpu.SMEM((NQB, NFAR), jnp.int32),
            dma((2,)),
            pltpu.VMEM((TOK, WIDTH), bf16),
            pltpu.VMEM((WIDTH, 2 * HEAD + QW), bf16),
            pltpu.VMEM((TP, QW, WIDTH), bf16),
            pltpu.VMEM((TOK, QW), bf16),
            piece,
            piece,
            [piece for _ in UP],
            [piece for _ in DOWN],
            pltpu.VMEM((GROUPS, NQB, KSPAN, HEAD), bf16),
            pltpu.VMEM((GROUPS, NQB, KSPAN, HEAD), bf16),
            pltpu.VMEM((arrivals * 2 * (NX - 1), NQB, KSPAN, HEAD), bf16),
            [pltpu.VMEM((NX, NQB, KSPAN, HEAD), bf16) for _ in range(2)],
            pltpu.VMEM((2 * (NX - 1), NQB, KSPAN, HEAD), bf16),
            [[pltpu.VMEM((FIRST, KSPAN, HEAD), bf16) for _ in range(NX - 1)] for _ in LATE],
            [pltpu.VMEM((NX, FIRST, KSPAN, HEAD), bf16) for _ in range(2)],
            pltpu.VMEM((2 * NX, NQB, 128), jnp.int32),
            pltpu.SMEM((2 * NX, NQB, 128), jnp.int32),
            pltpu.VMEM((2, LISTED, HEAD), bf16),
            pltpu.VMEM((2, LISTED, HEAD), bf16),
            pltpu.VMEM((TP, SPAN, QW), bf16),
            pltpu.VMEM((TP, SPAN, QW), bf16),
            pltpu.VMEM((SPAN, WIDTH), jnp.float32),
            dma((NCHUNK,)), dma((3,)), dma((1,)), dma((3 * NX,)), dma((2 * NX,)), dma((2 * NX,)),
            dma((2, HALF + 1)), dma((2, HALF + 1)), dma((2, HALF + 1)), dma((2, HALF + 1)),
            dma((arrivals, 2, NX - 1)), dma((arrivals, 2, NX - 1)),
            dma((len(LATE), NX - 1)), dma((len(LATE), NX - 1)), dma((2, NX)), dma((2, NX)), dma((2,)), dma((2,)),
            dma((4,)), dma((4,)), dma((5,)), dma((5,)), dma((TP,)), dma((TP,)),
        ],
        compiler_params=pltpu.CompilerParams(
            collective_id=0, has_side_effects=True, vmem_limit_bytes=56 * 2**20
        ),
        name="sparse_attention_layer",
    )(tokens, query_weight, key_projection_matrix, value_projection_matrix, out_weight, chosen)


def solution(mesh):
    return jax.shard_map(
        shards,
        mesh=mesh,
        in_specs=(
            P("kv", None),
            P(None, "tp"),
            P(None, "tp"),
            P(None, "tp"),
            P("tp", None),
            P("kv", None),
        ),
        out_specs=P(("kv", "tp"), None),
        check_vma=False,
    )
```
